32 devices in a mesh: sp: 8 (over z, y), tp: 4 (over x, core).
Axes of the slice: x: 2, y: 2, z: 4, core: 2. Of those that a mesh axis runs over, the one named last changes fastest.
Arguments:
- out_cotangent: bfloat16 [1024, 2048], P('sp', 'tp'), may hold values from -6 to 6
- expert_input: bfloat16 [1024, 2048], P('sp', 'tp'), may hold values from -6 to 6
- routes: int32 [1024, 2], P('sp'), may hold values from 0 to 7, as said below
- route_weights: float32 [1024, 2], P('sp'), may hold values from 0.2 to 1
- gate_proj: bfloat16 [8, 2048, 3584], P('sp', None, 'tp'), may hold values from -0.125 to 0.125
- up_proj: bfloat16 [8, 2048, 3584], P('sp', None, 'tp'), may hold values from -0.125 to 0.125
- down_proj: bfloat16 [8, 3584, 2048], P('sp', 'tp'), may hold values from -0.09375 to 0.09375
- conv_out: bfloat16 [1024, 2048], P('sp', 'tp'), may hold values from -27 to 27
- conv_mean: float32 [1024], P('sp'), may hold values from -3 to 3
- conv_rstd: float32 [1024], P('sp'), may hold values from 0.25 to 1
- norm_gain: float32 [2048], P('tp'), may hold values from 0.1 to 1.9
- taps: float32 [31, 2048], P(None, 'tp'), may hold values from -1 to 1
- out_proj: bfloat16 [2048, 2048], P(None, 'tp'), may hold values from -0.125 to 0.125
Outputs:
- gate_grad: bfloat16 [8, 2048, 3584], P('sp', None, 'tp')
- up_grad: bfloat16 [8, 2048, 3584], P('sp', None, 'tp')
- down_grad: bfloat16 [8, 3584, 2048], P('sp', 'tp')
- proj_grad: float32 [2048, 2048], P('sp', 'tp')
- stream_grad: bfloat16 [1024, 2048], P('sp', 'tp')
- conv_in_grad: bfloat16 [1024, 2048], P('sp', 'tp')
The draws below stay inside these ranges and needn't reach their ends.
Inputs may be any that keep to these rules, and one draw needn't show every extreme that they name: `routes`: each row names 2 different experts. In each aligned block of 128 rows (the rows of one device) no expert is named by more than 48 rows, and one expert, the same in every block, is named by exactly 48 rows of every block.
All inputs are finite; a program needn't handle non-finite values.
Results may differ from the reference program's by a relative error of at most 0.02.
Values may be sent and summed in bfloat16 or wider, within the bound.
A program may use at most 128 MiB of HBM per device.

```python
import math
import jax
import jax.numpy as jnp
from jax import lax

D = 2048
FF = 3584
TOP = 2
TAPS = 31
TOK_DEV = 128
EXPERTS = 8
CAP = 48
TOKENS = 1024
HID_BLOCKS = 4


def draw_routes(key, part):
    blocks = TOKENS // TOK_DEV
    hot_key, rest_key = jax.random.split(jax.random.fold_in(key, 11))
    hottest = jax.random.randint(hot_key, (), 0, EXPERTS).astype(jnp.int32)
    block_keys = jax.random.split(rest_key, blocks)
    spare = 2 * TOK_DEV - CAP
    base_count = spare // (EXPERTS - 1)
    extra_count = spare % (EXPERTS - 1)
    shift_reach = min(base_count, CAP - base_count - 1)
    pair_count = (EXPERTS - 1) // 2

    def one_block(block_key):
        perm_key, shift_key, row_key, side_key = jax.random.split(block_key, 4)
        others = jax.random.permutation(perm_key, EXPERTS - 1).astype(jnp.int32)
        others = others + (others >= hottest).astype(jnp.int32)
        expert_order = jnp.concatenate([hottest[None], others])
        counts = base_count + (jnp.arange(EXPERTS - 1) < extra_count).astype(jnp.int32)
        moves = jax.random.randint(shift_key, (pair_count,), 0, shift_reach + 1).astype(jnp.int32)
        change = jnp.concatenate([jnp.stack([moves, -moves], axis=1).reshape(-1), jnp.zeros((EXPERTS - 1 - 2 * pair_count,), jnp.int32)])
        counts = jnp.concatenate([jnp.full((1,), CAP, jnp.int32), counts + change])
        run_ends = jnp.cumsum(counts)
        position = jnp.arange(2 * TOK_DEV, dtype=jnp.int32)
        run_index = jnp.sum((position[:, None] >= run_ends[None, :]).astype(jnp.int32), axis=1)
        labels = expert_order[run_index]
        first_half = labels[:TOK_DEV]
        second_half = labels[TOK_DEV:]
        row_order = jax.random.permutation(row_key, TOK_DEV)
        flipped = jax.random.randint(side_key, (TOK_DEV,), 0, 2)
        left_col = jnp.where(flipped == 1, second_half, first_half)[row_order]
        right_col = jnp.where(flipped == 1, first_half, second_half)[row_order]
        return jnp.stack([left_col, right_col], axis=1)
    return jax.vmap(one_block)(block_keys).reshape(TOKENS, TOP).astype(jnp.int32)


def draw_conv_out(key, part):
    noise_key, rough_key = jax.random.split(jax.random.fold_in(key, 23))
    channel = jnp.arange(D, dtype=jnp.float32)
    rising = jnp.exp(jnp.log(3.0) * channel / (D - 1))
    rough = jax.random.uniform(rough_key, (D,), jnp.float32, 0.6, 1.5)
    values = jnp.clip(jax.random.normal(noise_key, (TOKENS, D), jnp.float32), -6.0, 6.0)
    return (values * rising[None, :] * rough[None, :]).astype(jnp.bfloat16)


def spiked(result, stream_key, source, target, shards_of, factor):
    owner, partner = [(jnp.arange(result.shape[dim]) // (result.shape[dim] // shards_of)).reshape([-1 if axis == dim else 1 for axis in range(result.ndim)]) for dim in (source, target)]
    chosen = jax.random.permutation(stream_key, shards_of)[partner]
    strong = (owner == chosen) | (owner == (partner + shards_of // 2) % shards_of)
    return jnp.where(strong, factor * result, result)


def levels(own_key, extent, pieces, smallest, largest):
    loudness, own = 1.0, jax.random.fold_in(own_key, 6)
    for axis_at, blocks in pieces:
        draws = jnp.exp(jax.random.uniform(jax.random.fold_in(own, axis_at), (blocks,), jnp.float32, smallest / len(pieces), largest / len(pieces)))
        loudness = loudness * jnp.repeat(draws, extent[axis_at] // blocks).reshape([-1 if axis == axis_at else 1 for axis in range(len(extent))])
    return loudness


def scatter_about(key, dims, deviation, bound, shards=(), kind=jnp.bfloat16):
    level = levels(key, dims, shards, -0.22, 0.18) if shards else 1.0
    drawn = jax.random.normal(key, dims, jnp.float32) * deviation * level
    return jnp.minimum(jnp.maximum(drawn, -bound), bound).astype(kind)


def noise_with(rng, dims, width, bound, cuts, heavy, kind=jnp.bfloat16):
    values = width * jax.random.normal(rng, dims, jnp.float32)
    if cuts:
        values = values * levels(rng, dims, cuts, -0.22, 0.18)
    return jnp.clip(spiked(values, jax.random.fold_in(rng, 3), *heavy), -bound, bound).astype(kind)


def setup_inputs(seed: int = 0) -> dict:
    splits = jax.random.split(jax.random.key(seed), 14)
    return {
        "out_cotangent": noise_with(splits[0], (TOKENS, D), 1.0, 6.0, ((0, 8), (1, 4)), (0, 1, 8, 2.0)),
        "expert_input": scatter_about(splits[1], (TOKENS, D), 1.0, 6.0, ((0, 8), (1, 4))),
        "routes": draw_routes(jax.random.fold_in(splits[13], 71), 0),
        "route_weights": jnp.clip(0.2 + 0.8 * jax.random.uniform(splits[3], (TOKENS, TOP), jnp.float32) ** levels(splits[3], (TOKENS, TOP), ((0, 8),), -0.2, 0.2), 0.2, 1.0),
        "gate_proj": scatter_about(splits[4], (EXPERTS, D, FF), D ** -0.5, 0.125, ((0, 8), (2, 4))),
        "up_proj": scatter_about(splits[5], (EXPERTS, D, FF), D ** -0.5, 0.125, ((0, 8), (2, 4))),
        "down_proj": scatter_about(splits[6], (EXPERTS, FF, D), FF ** -0.5, 0.09375, ((0, 8), (1, 4))),
        "conv_out": draw_conv_out(jax.random.fold_in(splits[13], 71), 0),
        "conv_mean": scatter_about(splits[8], (TOKENS,), 0.5, 3.0, ((0, 8),), jnp.float32),
        "conv_rstd": jnp.clip(jnp.exp(math.log(1.0) - 1.3862944 * jax.random.uniform(splits[9], (TOKENS,), jnp.float32) ** levels(splits[9], (TOKENS,), ((0, 8),), -0.2, 0.2)), 0.25, 1.0),
        "norm_gain": jnp.clip(1.0 + 0.18 * jax.random.normal(splits[10], (D,), jnp.float32), 0.1, 1.9),
        "taps": scatter_about(splits[11], (TAPS, D), TAPS ** -0.5, 1.0, ((1, 4),), jnp.float32),
        "out_proj": scatter_about(splits[12], (D, D), D ** -0.5, 0.125, ((1, 4),)),
    }


OUTER_DIMS = (((0,), (0,)), ((), ()))
INNER_DIMS = (((1,), (1,)), ((), ()))


def reference(out_cotangent, expert_input, routes, route_weights, gate_proj, up_proj, down_proj, conv_out, conv_mean, conv_rstd, norm_gain, taps, out_proj):
    assigned = routes.reshape(-1).astype(jnp.int32)
    pair_weights = route_weights.reshape(-1)
    limit = CAP * EXPERTS
    outside = TOKENS * TOP
    block_width = FF // HID_BLOCKS

    def one_expert(expert_id):
        picked = jnp.nonzero(assigned == expert_id, size=limit, fill_value=outside)[0].astype(jnp.int32)
        usable = picked < outside
        safe_pair = jnp.where(usable, picked, 0)
        token_index = safe_pair // TOP
        rows = jnp.where(usable[:, None], expert_input[token_index], jnp.zeros((), jnp.bfloat16))
        weight = jnp.where(usable, pair_weights[safe_pair], 0.0)
        routed_cot = (weight[:, None] * out_cotangent[token_index].astype(jnp.float32)).astype(jnp.bfloat16)
        gate_local = gate_proj[expert_id]
        up_local = up_proj[expert_id]
        down_local = down_proj[expert_id]
        gate_pre = jnp.dot(rows, gate_local, preferred_element_type=jnp.float32)
        up_pre = jnp.dot(rows, up_local, preferred_element_type=jnp.float32)
        gate_sigmoid = jax.nn.sigmoid(gate_pre)
        activation = (gate_pre * gate_sigmoid * up_pre).astype(jnp.bfloat16)
        act_grad = lax.dot_general(routed_cot, down_local, INNER_DIMS, preferred_element_type=jnp.float32)
        gate_back = (act_grad * up_pre * gate_sigmoid * (1.0 + gate_pre * (1.0 - gate_sigmoid))).astype(jnp.bfloat16)
        up_back = (act_grad * gate_pre * gate_sigmoid).astype(jnp.bfloat16)
        down_part = lax.dot_general(activation, routed_cot, OUTER_DIMS, preferred_element_type=jnp.float32).astype(jnp.bfloat16)
        gate_part = lax.dot_general(rows, gate_back, OUTER_DIMS, preferred_element_type=jnp.float32).astype(jnp.bfloat16)
        up_part = lax.dot_general(rows, up_back, OUTER_DIMS, preferred_element_type=jnp.float32).astype(jnp.bfloat16)
        block_parts = jnp.einsum('lbu,dbu->lbd', gate_back.astype(jnp.float32).reshape(limit, HID_BLOCKS, block_width), gate_local.astype(jnp.float32).reshape(D, HID_BLOCKS, block_width))
        block_parts = block_parts + jnp.einsum('lbu,dbu->lbd', up_back.astype(jnp.float32).reshape(limit, HID_BLOCKS, block_width), up_local.astype(jnp.float32).reshape(D, HID_BLOCKS, block_width))
        block_parts = block_parts.astype(jnp.bfloat16)
        routed_grad = jnp.sum(block_parts.astype(jnp.float32), axis=1).astype(jnp.bfloat16)
        return gate_part, up_part, down_part, routed_grad, picked

    gate_grad, up_grad, down_grad, routed_grad, picked = lax.map(one_expert, jnp.arange(EXPERTS, dtype=jnp.int32))
    placed = jnp.zeros((outside, D), jnp.bfloat16).at[picked.reshape(-1)].set(routed_grad.reshape(-1, D), mode="drop")
    routed_sum = jnp.sum(placed.reshape(TOKENS, TOP, D).astype(jnp.float32), axis=1)
    stream_grad = (out_cotangent.astype(jnp.float32) + routed_sum).astype(jnp.bfloat16)

    normed = (conv_out.astype(jnp.float32) - conv_mean[:, None]) * conv_rstd[:, None]
    scaled = normed * norm_gain[None, :]
    scaled_sigmoid = jax.nn.sigmoid(scaled)
    swished = (scaled * scaled_sigmoid).astype(jnp.bfloat16)
    proj_grad = lax.dot_general(stream_grad, swished, OUTER_DIMS, preferred_element_type=jnp.float32)
    swished_grad = jnp.dot(stream_grad, out_proj, preferred_element_type=jnp.float32)
    scaled_grad = swished_grad * scaled_sigmoid * (1.0 + scaled * (1.0 - scaled_sigmoid)) * norm_gain[None, :]
    first_mean = jnp.mean(scaled_grad, axis=1, keepdims=True)
    second_mean = jnp.mean(scaled_grad * normed, axis=1, keepdims=True)
    conv_grad = conv_rstd[:, None] * (scaled_grad - first_mean - normed * second_mean)
    padded = jnp.concatenate([conv_grad, jnp.zeros((TAPS - 1, D), jnp.float32)], axis=0)
    conv_sum = jnp.zeros((TOKENS, D), jnp.float32)
    for offset in range(TAPS):
        conv_sum = conv_sum + taps[offset][None, :] * padded[offset:offset + TOKENS]
    return gate_grad, up_grad, down_grad, proj_grad, stream_grad, conv_sum.astype(jnp.bfloat16)
```

```python
import functools

import jax
import jax.numpy as jnp
from jax import lax
from jax.experimental import pallas as pl
from jax.experimental.pallas import tpu as pltpu
from jax.sharding import PartitionSpec as P

OUTER_DIMS = (((0,), (0,)), ((), ()))
INNER_DIMS = (((1,), (1,)), ((), ()))
MESH = pl.DeviceIdType.MESH
VMEM = pltpu.VMEM


def flipped(index, bit):
    return index + bit - 2 * bit * ((index // bit) % 2)


def masked(index, mask):
    for bit in bits_of(mask + 1):
        if mask & bit:
            index = flipped(index, bit)
    return index


def bits_of(count):
    bits, bit = [], 1
    while bit < count:
        bits.append(bit)
        bit *= 2
    return bits


def greet(devices):
    barrier = pltpu.get_barrier_semaphore()
    for device in devices:
        pl.semaphore_signal(barrier, inc=1, device_id=device, device_id_type=MESH)
    pl.semaphore_wait(barrier, len(devices))


def remote(src, dst, send_sem, recv_sem, device):
    return pltpu.make_async_remote_copy(
        src_ref=src, dst_ref=dst, send_sem=send_sem, recv_sem=recv_sem,
        device_id=device, device_id_type=MESH,
    )


def dispatch_kernel(
    experts, parts, rows_send_ref, cot_send_ref, rows_ref, cot_ref,
    out_send, out_recv, hop_send, hop_recv, local_sem,
):
    me, col = lax.axis_index("sp"), lax.axis_index("tp")
    width = rows_send_ref.shape[2]
    bits = bits_of(parts)[::-1]
    greet(
        [(lax.rem(me + k, experts), col) for k in range(1, experts)]
        + [(me, flipped(col, bit)) for bit in bits]
    )
    sends, fulls = (rows_send_ref, cot_send_ref), (rows_ref, cot_ref)

    def place(kind, source, column):
        return fulls[kind].at[source, :, pl.ds(pl.multiple_of(column * width, width), width)]

    def out_copy(kind, peer):
        return remote(
            sends[kind].at[peer], place(kind, me, col), out_send.at[kind, peer],
            out_recv.at[kind, me], (peer, col),
        )

    own = []
    for kind in range(2):
        own.append(
            pltpu.make_async_copy(sends[kind].at[me], place(kind, me, col), local_sem.at[kind])
        )
        own[kind].start()
    for kind in range(2):
        for mask in range(1, experts):
            out_copy(kind, masked(me, mask)).start()
    for copy in own:
        copy.wait()

    held = [[col]]
    for bit in bits:
        held.append(held[-1] + [flipped(column, bit) for column in held[-1]])
    starts, total = [], 0
    for level in range(len(bits)):
        starts.append(total)
        total += len(held[level])

    def hop(kind, level, slot, column, source):
        index = starts[level] + slot
        return remote(
            place(kind, source, column), place(kind, source, column),
            hop_send.at[kind, index, source], hop_recv.at[kind, index, source],
            (me, flipped(col, bits[level])),
        )

    def hop_arrival(kind, level, slot, source):
        return hop(kind, level, slot, flipped(held[level][slot], bits[level]), source)

    pieces = [(kind, mask) for kind in range(2) for mask in range(experts)]
    for kind, mask in [(0, 0), (1, 0)] + [piece for piece in pieces if piece[1]]:
        source = masked(me, mask)
        if mask:
            remote(
                sends[kind].at[source], place(kind, source, col), out_send.at[kind, source],
                out_recv.at[kind, source], (source, col),
            ).wait_recv()
        for level in range(len(bits)):
            hop(kind, level, 0, col, source).start()
    for level in range(1, len(bits)):
        size = len(held[level - 1])
        for kind, mask in pieces:
            source = masked(me, mask)
            for slot in range(size):
                hop_arrival(kind, level - 1, slot, source).wait_recv()
            for later in range(level, len(bits)):
                for slot in range(size, 2 * size):
                    hop(kind, later, slot, held[level][slot], source).start()

    for kind in range(2):

        def finish(k, carry, kind=kind):
            source = lax.rem(me + k, experts)
            last = len(bits) - 1
            for slot in range(len(held[last])):
                hop_arrival(kind, last, slot, source).wait_recv()
            for level in range(len(bits)):
                for slot in range(len(held[level])):
                    hop(kind, level, slot, held[level][slot], source).wait_send()

            @pl.when(k > 0)
            def _():
                out_copy(kind, source).wait_send()

            return carry

        lax.fori_loop(0, experts, finish, 0)


def dispatch(rows_send, cot_send, experts, parts):
    _, capacity, width = rows_send.shape
    hops = parts - 1
    full = jax.ShapeDtypeStruct((experts, capacity, width * parts), jnp.bfloat16)
    return pl.pallas_call(
        functools.partial(dispatch_kernel, experts, parts),
        out_shape=(full, full),
        in_specs=[pl.BlockSpec(memory_space=VMEM)] * 2,
        out_specs=[pl.BlockSpec(memory_space=VMEM)] * 2,
        scratch_shapes=[pltpu.SemaphoreType.DMA((2, experts))] * 2
        + [pltpu.SemaphoreType.DMA((2, hops, experts))] * 2
        + [pltpu.SemaphoreType.DMA((2,))],
        compiler_params=pltpu.CompilerParams(collective_id=0, has_side_effects=True),
        name="dispatch",
    )(rows_send, cot_send)


def column_of(row, rows):
    return jnp.broadcast_to(row, (128, rows)).T[:, 0:1]


def combine_kernel(
    experts, parts, partial_ref, conv_out_ref, mean_ref, rstd_ref, gain_ref, routed_ref, near_ref,
    *rest,
):
    bits = bits_of(parts)
    levels = len(bits)
    recv_bufs = rest[:levels]
    work, final = rest[levels], rest[levels + 1]
    hop_send, hop_recv, out_send, out_recv, sw_send, sw_recv = rest[levels + 2 :]
    me, col = lax.axis_index("sp"), lax.axis_index("tp")
    width = routed_ref.shape[2]
    greet(
        [(lax.rem(me + k, experts), col) for k in range(1, experts)]
        + [(me, flipped(col, bit)) for bit in bits]
    )
    tokens = conv_out_ref.shape[0]

    kept = [[col]]
    for bit in reversed(bits):
        kept.insert(0, kept[0] + [flipped(column, bit) for column in kept[0]])
    starts, total = [], 0
    for level in range(levels):
        starts.append(total)
        total += len(kept[level + 1])

    def columns(column):
        return pl.ds(pl.multiple_of(column * width, width), width)

    def hop(level, slot, block):
        column = flipped(kept[level + 1][slot], bits[level])
        index = starts[level] + slot
        if level == 0:
            src = partial_ref.at[block, :, columns(column)]
        else:
            src = work.at[level - 1, slot, block]
        return remote(
            src, recv_bufs[level].at[slot, block], hop_send.at[index, block],
            hop_recv.at[index, block], (me, flipped(col, bits[level])),
        )

    def summed(level, slot_column, slot_path, block):
        value = partial_ref[block, :, columns(slot_column)].astype(jnp.float32)
        for stage in range(level):
            value = value + recv_bufs[stage][slot_path[stage], block].astype(jnp.float32)
        return value

    def block_of(k):
        return lax.rem(me + k, experts)

    def start_first(k, carry):
        for slot in range(len(kept[1])):
            hop(0, slot, block_of(k)).start()
        return carry

    lax.fori_loop(1, experts + 1, start_first, 0)

    scaled = (
        (conv_out_ref[...].astype(jnp.float32) - column_of(mean_ref[...], tokens))
        * column_of(rstd_ref[...], tokens)
        * gain_ref[...]
    )
    near_ref[me // 2] = (scaled * jax.nn.sigmoid(scaled)).astype(jnp.bfloat16)

    far_bits = bits_of(experts)[:0:-1]
    sources = [[me]]
    for bit in far_bits:
        sources.append(sources[-1] + [flipped(source, bit) for source in sources[-1]])

    def sw_copy(level, slot, source):
        index = (1 << level) - 1 + slot
        return remote(
            near_ref.at[source // 2], near_ref.at[source // 2], sw_send.at[index],
            sw_recv.at[index], (flipped(me, far_bits[level]), col),
        )

    def sw_start(level):
        for slot, source in enumerate(sources[level]):
            sw_copy(level, slot, source).start()

    def sw_arrive(level):
        for slot, source in enumerate(sources[level]):
            sw_copy(level, slot, flipped(source, far_bits[level])).wait_recv()

    for level in range(1, levels):

        def middle(k, carry, level=level):
            block = block_of(k)
            for slot in range(len(kept[level])):
                hop(level - 1, slot, block).wait_recv()
            size = len(kept[level + 1])
            for slot in range(size):
                value = summed(
                    level, kept[level][size + slot], [size + slot] * level, block
                )
                work[level - 1, slot, block] = value.astype(jnp.bfloat16)
            for slot in range(size):
                hop(level, slot, block).start()
            return carry

        lax.fori_loop(1, experts + 1, middle, 0)

    sw_start(0)

    def out_copy(block):
        return remote(
            final.at[block], routed_ref.at[me], out_send.at[block], out_recv.at[me], (block, col)
        )

    def last(k, carry):
        block = block_of(k)
        hop(levels - 1, 0, block).wait_recv()
        value = summed(levels, col, [0] * levels, block).astype(jnp.bfloat16)

        @pl.when(k < experts)
        def _():
            final[block] = value
            out_copy(block).start()

        @pl.when(k == experts)
        def _():
            routed_ref[me] = value

        return carry

    lax.fori_loop(1, experts + 1, last, 0)
    for level in range(len(far_bits)):
        sw_arrive(level)
        if level + 1 < len(far_bits):
            sw_start(level + 1)

    def finish(k, carry):
        block = block_of(k)
        for level in range(levels):
            for slot in range(len(kept[level + 1])):
                hop(level, slot, block).wait_send()

        @pl.when(k < experts)
        def _():
            out_copy(block).wait_send()
            remote(
                final.at[block], routed_ref.at[block], out_send.at[block],
                out_recv.at[block], (block, col),
            ).wait_recv()

        return carry

    lax.fori_loop(1, experts + 1, finish, 0)
    for level in range(len(far_bits)):
        for slot, source in enumerate(sources[level]):
            sw_copy(level, slot, source).wait_send()


def combine(partial, conv_out, mean, rstd, gain, experts, parts):
    _, capacity, full = partial.shape
    width = full // parts
    levels = len(bits_of(parts))
    hops = parts - 1
    recv = [
        VMEM((parts >> (level + 1), experts, capacity, width), jnp.bfloat16)
        for level in range(levels)
    ]
    return pl.pallas_call(
        functools.partial(combine_kernel, experts, parts),
        out_shape=(
            jax.ShapeDtypeStruct((experts, capacity, width), jnp.bfloat16),
            jax.ShapeDtypeStruct((experts // 2,) + conv_out.shape, jnp.bfloat16),
        ),
        in_specs=[pl.BlockSpec(memory_space=VMEM)] * 5,
        out_specs=[pl.BlockSpec(memory_space=VMEM)] * 2,
        scratch_shapes=recv
        + [
            VMEM((max(levels - 1, 1), max(parts // 4, 1), experts, capacity, width), jnp.bfloat16),
            VMEM((experts, capacity, width), jnp.bfloat16),
            pltpu.SemaphoreType.DMA((hops, experts)),
            pltpu.SemaphoreType.DMA((hops, experts)),
            pltpu.SemaphoreType.DMA((experts,)),
            pltpu.SemaphoreType.DMA((experts,)),
            pltpu.SemaphoreType.DMA((experts // 2,)),
            pltpu.SemaphoreType.DMA((experts // 2,)),
        ],
        compiler_params=pltpu.CompilerParams(collective_id=1, has_side_effects=True),
        name="combine",
    )(partial, conv_out, mean, rstd, gain)


def tail_kernel(
    experts, parts, stream_ref, conv_out_ref, mean_ref, rstd_ref, gain_ref, taps_ref, proj_ref,
    near_ref, conv_ref, proj_grad_ref,
    whole, arrived, far, extended, stats, grads, norms,
    hop_send, hop_recv, out_send, out_recv, stat_send, stat_recv, halo_sem, local_sem, far_sem,
):
    me, col = lax.axis_index("sp"), lax.axis_index("tp")
    width, rows = stream_ref.shape
    full = width * parts
    block = full // experts
    bits = bits_of(parts)[::-1]
    tap_count = taps_ref.shape[0]
    halo = extended.shape[0] - rows
    greet(
        [(lax.rem(me + k, experts), col) for k in range(1, experts)]
        + [(me, lax.rem(col + k, parts)) for k in range(1, parts)]
    )

    far_copy = remote(near_ref, far, far_sem.at[0], far_sem.at[1], (flipped(me, 1), col))
    far_copy.start()

    def part(column):
        return whole.at[pl.ds(pl.multiple_of(column * width, width), width), :]

    own = pltpu.make_async_copy(stream_ref, part(col), local_sem.at[0])
    own.start()
    index, held, copies = 0, [col], []
    for level, bit in enumerate(bits):
        for slot, column in enumerate(held):
            src = stream_ref if column is col else part(column)
            copy = remote(
                src, part(column), hop_send.at[index + slot], hop_recv.at[index + slot],
                (me, flipped(col, bit)),
            )
            copy.start()
            copies.append(copy)
        for slot in range(len(held)):
            column = flipped(held[slot], bit)
            remote(
                part(column), part(column), hop_send.at[index + slot], hop_recv.at[index + slot],
                (me, flipped(col, bit)),
            ).wait_recv()
        index += len(held)
        held = held + [flipped(column, bit) for column in held]
    own.wait()

    def piece(peer):
        return whole.at[pl.ds(pl.multiple_of(peer * block, block), block), :]

    def landing(receiver, source):
        slot = lax.rem(receiver + source, 2) * (experts // 2) + source // 2
        return arrived.at[:, pl.ds(pl.multiple_of(slot * rows, rows), rows)]

    def out_copy(peer):
        return remote(piece(peer), landing(peer, me), out_send.at[peer], out_recv.at[me], (peer, col))

    def start_out(k, carry):
        out_copy(lax.rem(me + k, experts)).start()
        return carry

    lax.fori_loop(1, experts, start_out, 0)
    mine = pltpu.make_async_copy(piece(me), landing(me, me), local_sem.at[1])
    mine.start()

    gain = gain_ref[...]
    rstd = column_of(rstd_ref[...], rows)
    swished_grad = lax.dot_general(
        whole[...], proj_ref[...], OUTER_DIMS, preferred_element_type=jnp.float32
    )
    normed = (conv_out_ref[...].astype(jnp.float32) - column_of(mean_ref[...], rows)) * rstd
    scaled = normed * gain
    sig = jax.nn.sigmoid(scaled)
    scaled_grad = swished_grad * sig * (1.0 + scaled * (1.0 - sig)) * gain
    grads[...] = scaled_grad
    norms[...] = normed
    first = jnp.sum(scaled_grad, axis=1, keepdims=True)
    second = jnp.sum(scaled_grad * normed, axis=1, keepdims=True)
    lane = lax.broadcasted_iota(jnp.int32, (rows, 128), 1)
    both = jnp.where(lane == 0, first, second)
    stats[parts] = both.T[:8]
    stat_copies = []
    for k in range(1, parts):
        copy = remote(
            stats.at[parts], stats.at[k], stat_send.at[k], stat_recv.at[k],
            (me, lax.rem(col + k, parts)),
        )
        copy.start()
        stat_copies.append(copy)
    for copy in stat_copies:
        copy.wait()
    total = stats[parts]
    for k in range(1, parts):
        total = total + stats[k]
    total = total / full
    spread = jnp.concatenate([total] * 16, axis=0).T
    first_mean = spread[:, 0:1]
    second_mean = spread[:, 1:2]
    extended[0:rows, :] = rstd * (grads[...] - first_mean - norms[...] * second_mean)

    def halo_copy(device):
        return remote(
            extended.at[pl.ds(0, halo), :], extended.at[pl.ds(rows, halo), :],
            halo_sem.at[0], halo_sem.at[1], (device, col),
        )

    @pl.when(me > 0)
    def _():
        halo_copy(lax.rem(me + experts - 1, experts)).start()

    @pl.when(me == experts - 1)
    def _():
        extended[rows:, :] = jnp.zeros((halo, width), jnp.float32)

    @pl.when(me < experts - 1)
    def _():
        halo_copy(lax.rem(me + experts - 1, experts)).wait_recv()

    for start in range(0, width, 128):
        cols = pl.ds(start, 128)
        total = jnp.zeros((rows, 128), jnp.float32)
        for offset in range(tap_count):
            total = total + taps_ref[offset : offset + 1, cols] * extended[pl.ds(offset, rows), cols]
        conv_ref[:, cols] = total.astype(jnp.bfloat16)

    def finish(k, carry):
        source = lax.rem(me - k + experts, experts)
        remote(
            piece(source), landing(me, source), out_send.at[source], out_recv.at[source], (source, col)
        ).wait_recv()
        out_copy(source).wait_send()
        return carry

    lax.fori_loop(1, experts, finish, 0)
    mine.wait()
    half = experts // 2 * rows
    proj_grad_ref[...] = jnp.dot(
        arrived[:, :half], near_ref[...].reshape(half, width), preferred_element_type=jnp.float32
    )
    far_copy.wait()
    proj_grad_ref[...] += jnp.dot(
        arrived[:, half:], far[...].reshape(half, width), preferred_element_type=jnp.float32
    )
    for copy in copies:
        copy.wait_send()

    @pl.when(me > 0)
    def _():
        halo_copy(lax.rem(me + experts - 1, experts)).wait_send()


def tail(stream_t, conv_out, mean, rstd, gain, taps, proj, near, experts, parts):
    width, rows = stream_t.shape
    full = width * parts
    block = full // experts
    halo = -(-(taps.shape[0] - 1) // 8) * 8
    return pl.pallas_call(
        functools.partial(tail_kernel, experts, parts),
        out_shape=(
            jax.ShapeDtypeStruct((rows, width), jnp.bfloat16),
            jax.ShapeDtypeStruct((block, width), jnp.float32),
        ),
        in_specs=[pl.BlockSpec(memory_space=VMEM)] * 8,
        out_specs=[pl.BlockSpec(memory_space=VMEM)] * 2,
        scratch_shapes=[
            VMEM((full, rows), jnp.bfloat16),
            VMEM((block, experts * rows), jnp.bfloat16),
            VMEM(near.shape, jnp.bfloat16),
            VMEM((rows + halo, width), jnp.float32),
            VMEM((parts + 1, 8, rows), jnp.float32),
            VMEM((rows, width), jnp.float32),
            VMEM((rows, width), jnp.float32),
            pltpu.SemaphoreType.DMA((parts - 1,)),
            pltpu.SemaphoreType.DMA((parts - 1,)),
            pltpu.SemaphoreType.DMA((experts,)),
            pltpu.SemaphoreType.DMA((experts,)),
            pltpu.SemaphoreType.DMA((parts,)),
            pltpu.SemaphoreType.DMA((parts,)),
            pltpu.SemaphoreType.DMA((2,)),
            pltpu.SemaphoreType.DMA((2,)),
            pltpu.SemaphoreType.DMA((2,)),
        ],
        compiler_params=pltpu.CompilerParams(collective_id=2, has_side_effects=True),
        name="tail",
    )(stream_t, conv_out, mean, rstd, gain, taps, proj, near)


def body(
    out_cotangent,
    expert_input,
    routes,
    route_weights,
    gate_proj,
    up_proj,
    down_proj,
    conv_out,
    conv_mean,
    conv_rstd,
    norm_gain,
    taps,
    out_proj,
):
    tok_rows, local_width = out_cotangent.shape
    experts = lax.axis_size("sp")
    parts = lax.axis_size("tp")
    capacity = 3 * tok_rows // experts
    full_width = local_width * parts
    slots = experts * capacity

    chosen = routes[:, :, None] == jnp.arange(experts, dtype=jnp.int32)[None, None, :]
    named = jnp.any(chosen, axis=1)
    weight = jnp.sum(jnp.where(chosen, route_weights[:, :, None], 0.0), axis=1)
    before = jnp.arange(tok_rows)[None, :] < jnp.arange(tok_rows)[:, None]
    rank = jnp.dot(
        before.astype(jnp.bfloat16), named.astype(jnp.bfloat16), preferred_element_type=jnp.float32
    ).astype(jnp.int32)
    rank = jnp.where(named, rank, -1)
    pick = rank.T[:, None, :] == jnp.arange(capacity, dtype=jnp.int32)[None, :, None]
    slot_weight = jnp.sum(jnp.where(pick, weight.T[:, None, :], 0.0), axis=2)
    pick = pick.astype(jnp.bfloat16).reshape(slots, tok_rows)
    send_rows = jnp.dot(pick, expert_input, preferred_element_type=jnp.float32).astype(jnp.bfloat16)
    send_cot = (
        jnp.dot(pick, out_cotangent, preferred_element_type=jnp.float32)
        * slot_weight.reshape(slots, 1)
    ).astype(jnp.bfloat16)
    arrived_rows, arrived_cot = dispatch(
        send_rows.reshape(experts, capacity, local_width),
        send_cot.reshape(experts, capacity, local_width),
        experts, parts,
    )
    rows_in = arrived_rows.reshape(slots, full_width)
    cot_in = arrived_cot.reshape(slots, full_width)
    mean, rstd, gain = conv_mean[None, :], conv_rstd[None, :], norm_gain[None, :]
    gate_local = gate_proj[0]
    up_local = up_proj[0]
    down_local = down_proj[0]
    gate_pre = jnp.dot(rows_in, gate_local, preferred_element_type=jnp.float32)
    up_pre = jnp.dot(rows_in, up_local, preferred_element_type=jnp.float32)
    gate_sigmoid = jax.nn.sigmoid(gate_pre)
    activation = (gate_pre * gate_sigmoid * up_pre).astype(jnp.bfloat16)
    act_grad = lax.dot_general(cot_in, down_local, INNER_DIMS, preferred_element_type=jnp.float32)
    gate_back = (act_grad * up_pre * gate_sigmoid * (1.0 + gate_pre * (1.0 - gate_sigmoid))).astype(
        jnp.bfloat16
    )
    up_back = (act_grad * gate_pre * gate_sigmoid).astype(jnp.bfloat16)
    down_grad = lax.dot_general(
        activation, cot_in, OUTER_DIMS, preferred_element_type=jnp.float32
    ).astype(jnp.bfloat16)[None]
    gate_grad = lax.dot_general(
        rows_in, gate_back, OUTER_DIMS, preferred_element_type=jnp.float32
    ).astype(jnp.bfloat16)[None]
    up_grad = lax.dot_general(
        rows_in, up_back, OUTER_DIMS, preferred_element_type=jnp.float32
    ).astype(jnp.bfloat16)[None]
    partial_rows = lax.dot_general(
        gate_back, gate_local, INNER_DIMS, preferred_element_type=jnp.float32
    )
    partial_rows = partial_rows + lax.dot_general(
        up_back, up_local, INNER_DIMS, preferred_element_type=jnp.float32
    )
    partial = partial_rows.astype(jnp.bfloat16).reshape(experts, capacity, full_width)
    routed, near = combine(partial, conv_out, mean, rstd, gain, experts, parts)
    routed = routed.reshape(slots, local_width)
    routed_sum = lax.dot_general(pick, routed, OUTER_DIMS, preferred_element_type=jnp.float32)
    stream = (out_cotangent.astype(jnp.float32) + routed_sum).astype(jnp.bfloat16)
    conv_in_grad, proj_grad = tail(
        stream.T, conv_out, mean, rstd, gain, taps, out_proj, near, experts, parts
    )
    return (gate_grad, up_grad, down_grad, proj_grad, stream, conv_in_grad)


def solution(mesh):
    in_specs = (
        P("sp", "tp"),
        P("sp", "tp"),
        P("sp", None),
        P("sp", None),
        P("sp", None, "tp"),
        P("sp", None, "tp"),
        P("sp", "tp", None),
        P("sp", "tp"),
        P("sp"),
        P("sp"),
        P("tp"),
        P(None, "tp"),
        P(None, "tp"),
    )
    out_specs = (
        P("sp", None, "tp"),
        P("sp", None, "tp"),
        P("sp", "tp", None),
        P("sp", "tp"),
        P("sp", "tp"),
        P("sp", "tp"),
    )
    return jax.shard_map(body, mesh=mesh, in_specs=in_specs, out_specs=out_specs, check_vma=False)
```

```python
import functools

import jax
import jax.numpy as jnp
from jax import lax
from jax.experimental import pallas as pl
from jax.experimental.pallas import tpu as pltpu
from jax.sharding import PartitionSpec as P

OUTER_DIMS = (((0,), (0,)), ((), ()))
INNER_DIMS = (((1,), (1,)), ((), ()))
MESH = pl.DeviceIdType.MESH
VMEM = pltpu.VMEM


def flipped(index, bit):
    return index + bit - 2 * bit * ((index // bit) % 2)


def masked(index, mask):
    for bit in bits_of(mask + 1):
        if mask & bit:
            index = flipped(index, bit)
    return index


def bits_of(count):
    bits, bit = [], 1
    while bit < count:
        bits.append(bit)
        bit *= 2
    return bits


def greet(devices):
    barrier = pltpu.get_barrier_semaphore()
    for device in devices:
        pl.semaphore_signal(barrier, inc=1, device_id=device, device_id_type=MESH)
    pl.semaphore_wait(barrier, len(devices))


def remote(src, dst, send_sem, recv_sem, device):
    return pltpu.make_async_remote_copy(
        src_ref=src, dst_ref=dst, send_sem=send_sem, recv_sem=recv_sem,
        device_id=device, device_id_type=MESH,
    )


def column_of(row, rows):
    return jnp.broadcast_to(row, (128, rows)).T[:, 0:1]


def ladder(experts):
    half = experts // 2
    return list(range(half, experts)) + list(range(1, half))


def front_kernel(
    experts, parts, rows_send_ref, cot_send_ref, pick_ref, cotangent_ref, conv_out_ref, mean_ref,
    rstd_ref, gain_ref, gate_hbm, up_hbm, down_hbm,
    rows_out, cot_out, act_out, gate_out, up_out, stream_ref, stream_t_ref, near_ref,
    gate, up, down, full, gate_pre, up_pre, act_grad, backs, partial, first_recv, recv, work, final,
    routed, out_send, out_recv, hop_send, hop_recv, first_sems, back_send, back_recv, home_send,
    home_recv, sw_send, sw_recv, weight_sem, save_sem, own_sem,
):
    me, col = lax.axis_index("sp"), lax.axis_index("tp")
    width = rows_send_ref.shape[1]
    capacity = rows_send_ref.shape[0] // experts
    hidden = gate.shape[1]
    tokens = conv_out_ref.shape[0]
    up_bits = bits_of(parts)
    bits = up_bits[::-1]
    levels = len(bits)
    loads = []
    for index, (src, dst) in enumerate(((gate_hbm, gate), (up_hbm, up), (down_hbm, down))):
        loads.append(pltpu.make_async_copy(src.at[0], dst, weight_sem.at[index]))
        loads[-1].start()
    greet(
        [(lax.rem(me + k, experts), col) for k in range(1, experts)]
        + [(me, flipped(col, bit)) for bit in bits]
    )
    sends = (rows_send_ref, cot_send_ref)

    def block_rows(source):
        return pl.ds(pl.multiple_of(source * capacity, capacity), capacity)

    def place(kind, source, column):
        return full.at[kind, column, block_rows(source), :]

    def out_copy(kind, peer, owner):
        return remote(
            sends[kind].at[block_rows(peer), :], place(kind, owner, col), out_send.at[kind, peer],
            out_recv.at[kind, owner], (peer, col),
        )

    for kind in range(2):
        for mask in range(1, experts):
            peer = masked(me, mask)
            out_copy(kind, peer, me).start()
    own = []
    for kind in range(2):
        own.append(
            pltpu.make_async_copy(
                sends[kind].at[block_rows(me), :], place(kind, me, col), own_sem.at[kind]
            )
        )
        own[kind].start()
    for copy in own:
        copy.wait()

    held = [[col]]
    for bit in bits:
        held.append(held[-1] + [flipped(column, bit) for column in held[-1]])
    starts, total = [], 0
    for level in range(levels):
        starts.append(total)
        total += len(held[level])

    def hop(kind, level, slot, column, source):
        index = starts[level] + slot
        return remote(
            place(kind, source, column), place(kind, source, column),
            hop_send.at[kind, index, source], hop_recv.at[kind, index, source],
            (me, flipped(col, bits[level])),
        )

    def hop_arrival(kind, level, slot, source):
        return hop(kind, level, slot, flipped(held[level][slot], bits[level]), source)

    def first_hops(kind, source):
        for level in range(levels):
            hop(kind, level, 0, col, source).start()

    def arrive(kind):
        for mask in range(1, experts):
            source = masked(me, mask)
            out_copy(kind, source, source).wait_recv()
            first_hops(kind, source)

    def pass_on(kind, masks, level):
        size = len(held[level - 1])
        for mask in masks:
            source = masked(me, mask)
            for slot in range(size):
                hop_arrival(kind, level - 1, slot, source).wait_recv()
            for later in range(level, levels):
                for slot in range(size, 2 * size):
                    hop(kind, later, slot, held[level][slot], source).start()

    def collect(kind):
        def step(k, carry):
            source = lax.rem(me + k, experts)
            for slot in range(len(held[levels - 1])):
                hop_arrival(kind, levels - 1, slot, source).wait_recv()
            return carry

        lax.fori_loop(0, experts, step, 0)

    for kind in range(2):
        first_hops(kind, me)

    scaled = (
        (conv_out_ref[...].astype(jnp.float32) - column_of(mean_ref[...], tokens))
        * column_of(rstd_ref[...], tokens)
        * gain_ref[...]
    )
    near_ref[me // 2] = (scaled * jax.nn.sigmoid(scaled)).astype(jnp.bfloat16)

    far_bits = bits_of(experts)[:0:-1]
    sources = [[me]]
    for bit in far_bits:
        sources.append(sources[-1] + [flipped(source, bit) for source in sources[-1]])

    def sw_copy(level, slot, source):
        index = (1 << level) - 1 + slot
        return remote(
            near_ref.at[source // 2], near_ref.at[source // 2], sw_send.at[index],
            sw_recv.at[index], (flipped(me, far_bits[level]), col),
        )

    def sw_start(level):
        for slot, source in enumerate(sources[level]):
            sw_copy(level, slot, source).start()

    def sw_arrive(level):
        for slot, source in enumerate(sources[level]):
            sw_copy(level, slot, flipped(source, far_bits[level])).wait_recv()

    arrive(0)
    arrive(1)
    sw_start(0)
    masks = list(range(experts))
    for level in range(1, levels):
        pass_on(0, masks, level)
    collect(0)

    def tiles(step):
        whole = hidden // 256

        def one(j, carry):
            step(pl.ds(pl.multiple_of(j * 256, 256), 256), 256)
            return carry

        lax.fori_loop(0, whole, one, 0)
        if hidden % 256:
            step(pl.ds(whole * 256, hidden % 256), hidden % 256)

    def joined(kind):
        return jnp.concatenate([full[kind, part] for part in range(parts)], axis=1)

    loads[0].wait()
    loads[1].wait()

    def pre(cols, size):
        rows = joined(0)
        gate_pre[:, cols] = jnp.dot(rows, gate[:, cols], preferred_element_type=jnp.float32)
        up_pre[:, cols] = jnp.dot(rows, up[:, cols], preferred_element_type=jnp.float32)

    tiles(pre)
    for level in range(1, levels):
        pass_on(1, masks, level)
    collect(1)
    loads[2].wait()

    def back(cols, size):
        act_grad[:, 0:size] = lax.dot_general(
            joined(1), down[cols, :], INNER_DIMS, preferred_element_type=jnp.float32
        )

        def chunk(k, carry):
            rows = block_rows(k)
            gates, ups, grad = gate_pre[rows, cols], up_pre[rows, cols], act_grad[rows, 0:size]
            sig = jax.nn.sigmoid(gates)
            silu = gates * sig
            backs[0, rows, cols] = (silu * ups).astype(jnp.bfloat16)
            backs[1, rows, cols] = (grad * ups * sig * (1.0 + gates * (1.0 - sig))).astype(
                jnp.bfloat16
            )
            backs[2, rows, cols] = (grad * silu).astype(jnp.bfloat16)
            return carry

        lax.fori_loop(0, experts, chunk, 0)

    tiles(back)
    saves = [
        pltpu.make_async_copy(full.at[0], rows_out, save_sem.at[0]),
        pltpu.make_async_copy(full.at[1], cot_out, save_sem.at[1]),
        pltpu.make_async_copy(backs.at[0], act_out, save_sem.at[2]),
        pltpu.make_async_copy(backs.at[1], gate_out, save_sem.at[3]),
        pltpu.make_async_copy(backs.at[2], up_out, save_sem.at[4]),
    ]

    kept = [[col]]
    for bit in bits:
        kept.insert(0, kept[0] + [flipped(column, bit) for column in kept[0]])
    order = ladder(experts) + [0]

    def first_copy(slot):
        return remote(
            partial.at[flipped(kept[1][slot], up_bits[0])], first_recv.at[slot],
            first_sems.at[0, slot], first_sems.at[1, slot], (me, flipped(col, up_bits[0])),
        )

    def fill(column):
        rows = pl.ds(pl.multiple_of(column * width, width), width)
        value = lax.dot_general(
            backs[1], gate[rows, :], INNER_DIMS, preferred_element_type=jnp.float32
        ) + lax.dot_general(
            backs[2], up[rows, :], INNER_DIMS, preferred_element_type=jnp.float32
        )
        partial[column] = value.astype(jnp.bfloat16)

    back_starts, total = [0], 0
    for level in range(1, levels):
        back_starts.append(total)
        total += len(kept[level + 1])

    def back_copy(level, slot, block):
        index = back_starts[level] + slot
        return remote(
            work.at[index, block_rows(block), :], recv.at[index, block_rows(block), :],
            back_send.at[index, block], back_recv.at[index, block],
            (me, flipped(col, up_bits[level])),
        )

    def summed(level, slot, block):
        rows = block_rows(block)
        value = partial[kept[level][slot], rows, :].astype(jnp.float32)
        value = value + first_recv[slot, rows, :].astype(jnp.float32)
        for stage in range(1, level):
            value = value + recv[back_starts[stage] + slot, rows, :].astype(jnp.float32)
        return value.astype(jnp.bfloat16)

    for slot in reversed(range(len(kept[1]))):
        fill(flipped(kept[1][slot], up_bits[0]))
        first_copy(slot).start()
        fill(kept[1][slot])
        first_copy(slot).wait_recv()
        size = len(kept[2]) if levels > 1 else 0
        if levels > 1 and slot >= size:
            for mask in order:
                block = masked(me, mask)
                work[back_starts[1] + slot - size, block_rows(block), :] = summed(1, slot, block)
                back_copy(1, slot - size, block).start()
    for copy in saves:
        copy.start()
    for level in range(2, levels):
        size = len(kept[level + 1])
        for mask in order:
            block = masked(me, mask)
            for slot in range(2 * size):
                back_copy(level - 1, slot, block).wait_recv()
            for slot in range(size):
                work[back_starts[level] + slot, block_rows(block), :] = summed(
                    level, size + slot, block
                )
                back_copy(level, slot, block).start()

    def home_copy(block, owner):
        return remote(
            final.at[block_rows(block), :], routed.at[block_rows(owner), :],
            home_send.at[block], home_recv.at[owner], (block, col),
        )

    for mask in order:
        block = masked(me, mask)
        if levels > 1:
            back_copy(levels - 1, 0, block).wait_recv()
        value = summed(levels, 0, block)
        if mask:
            final[block_rows(block), :] = value
            home_copy(block, me).start()
        else:
            routed[block_rows(block), :] = value
    for level in range(len(far_bits)):
        sw_arrive(level)
        if level + 1 < len(far_bits):
            sw_start(level + 1)
    for mask in order[:-1]:
        source = masked(me, mask)
        home_copy(source, source).wait_recv()
    stream = cotangent_ref[...].astype(jnp.float32) + jnp.dot(
        pick_ref[...], routed[...], preferred_element_type=jnp.float32
    )
    stream_ref[...] = stream.astype(jnp.bfloat16)
    stream_t_ref[...] = stream.T.astype(jnp.bfloat16)

    def finish(k, carry):
        source = lax.rem(me + k, experts)
        for kind in range(2):
            for level in range(levels):
                for slot in range(len(held[level])):
                    hop(kind, level, slot, held[level][slot], source).wait_send()
        for level in range(1, levels):
            for slot in range(len(kept[level + 1])):
                back_copy(level, slot, source).wait_send()

        @pl.when(k > 0)
        def _():
            for kind in range(2):
                out_copy(kind, source, me).wait_send()
            home_copy(source, me).wait_send()

        return carry

    lax.fori_loop(0, experts, finish, 0)
    for slot in range(len(kept[1])):
        first_copy(slot).wait_send()
    for level in range(len(far_bits)):
        for slot, source in enumerate(sources[level]):
            sw_copy(level, slot, source).wait_send()
    for copy in saves:
        copy.wait()


def front(
    rows_send, cot_send, pick_t, cotangent, conv_out, mean, rstd, gain, gate, up, down, experts, parts
):
    slots, width = rows_send.shape
    full_width, hidden = gate.shape[1:]
    tokens = conv_out.shape[0]
    hops = parts - 1
    extra = max(parts // 2 - 1, 1)
    bf16, dma = jnp.bfloat16, pltpu.SemaphoreType.DMA
    rows_all = jax.ShapeDtypeStruct((parts, slots, width), bf16)
    acts = jax.ShapeDtypeStruct((slots, hidden), bf16)
    return pl.pallas_call(
        functools.partial(front_kernel, experts, parts),
        out_shape=(
            rows_all, rows_all, acts, acts, acts,
            jax.ShapeDtypeStruct((tokens, width), bf16),
            jax.ShapeDtypeStruct((width, tokens), bf16),
            jax.ShapeDtypeStruct((experts // 2, tokens, width), bf16),
        ),
        in_specs=[pl.BlockSpec(memory_space=VMEM)] * 8 + [pl.BlockSpec(memory_space=pl.ANY)] * 3,
        out_specs=[pl.BlockSpec(memory_space=pl.ANY)] * 5
        + [pl.BlockSpec(memory_space=VMEM)] * 3,
        scratch_shapes=[
            VMEM((full_width, hidden), bf16),
            VMEM((full_width, hidden), bf16),
            VMEM((hidden, full_width), bf16),
            VMEM((2, parts, slots, width), bf16),
            VMEM((slots, hidden), jnp.float32),
            VMEM((slots, hidden), jnp.float32),
            VMEM((slots, 256), jnp.float32),
            VMEM((3, slots, hidden), bf16),
            VMEM((parts, slots, width), bf16),
            VMEM((max(parts // 2, 1), slots, width), bf16),
            VMEM((extra, slots, width), bf16),
            VMEM((extra, slots, width), bf16),
            VMEM((slots, width), bf16),
            VMEM((slots, width), bf16),
            dma((2, experts)),
            dma((2, experts)),
            dma((2, hops, experts)),
            dma((2, hops, experts)),
            dma((2, max(parts // 2, 1))),
            dma((extra, experts)),
            dma((extra, experts)),
            dma((experts,)),
            dma((experts,)),
            dma((experts // 2,)),
            dma((experts // 2,)),
            dma((3,)),
            dma((5,)),
            dma((2,)),
        ],
        compiler_params=pltpu.CompilerParams(
            collective_id=0, has_side_effects=True, vmem_limit_bytes=50 * 1024 * 1024
        ),
        name="front",
    )(rows_send, cot_send, pick_t, cotangent, conv_out, mean, rstd, gain, gate, up, down)


def grads_kernel(rows_ref, cot_ref, act_ref, gate_ref, up_ref, gate_out, up_out, down_out):
    rows = rows_ref[...]
    gate_out[...] = lax.dot_general(
        rows, gate_ref[...], OUTER_DIMS, preferred_element_type=jnp.float32
    ).astype(jnp.bfloat16)
    up_out[...] = lax.dot_general(
        rows, up_ref[...], OUTER_DIMS, preferred_element_type=jnp.float32
    ).astype(jnp.bfloat16)
    down_out[...] = lax.dot_general(
        act_ref[...], cot_ref[...], OUTER_DIMS, preferred_element_type=jnp.float32
    ).astype(jnp.bfloat16)


def grads(rows, cot, act, gate_back, up_back):
    parts, slots, width = rows.shape
    hidden = act.shape[1]
    piece = pl.BlockSpec((None, slots, width), lambda i: (i, 0, 0))
    acts = pl.BlockSpec((slots, hidden), lambda i: (0, 0))
    across = pl.BlockSpec((None, width, hidden), lambda i: (0, i, 0))
    tall = jax.ShapeDtypeStruct((1, width * parts, hidden), jnp.bfloat16)
    return pl.pallas_call(
        grads_kernel,
        grid=(parts,),
        out_shape=(tall, tall, jax.ShapeDtypeStruct((1, hidden, width * parts), jnp.bfloat16)),
        in_specs=[piece, piece, acts, acts, acts],
        out_specs=[across, across, pl.BlockSpec((None, hidden, width), lambda i: (0, 0, i))],
        name="grads",
    )(rows, cot, act, gate_back, up_back)


def tail_kernel(
    experts, parts, stream_ref, conv_out_ref, mean_ref, rstd_ref, gain_ref, taps_ref, proj_ref,
    near_ref, conv_ref, proj_grad_ref,
    whole, arrived, far, extended, stats, grads, norms,
    hop_send, hop_recv, out_send, out_recv, stat_send, stat_recv, halo_sem, local_sem, far_sem,
):
    me, col = lax.axis_index("sp"), lax.axis_index("tp")
    width, rows = stream_ref.shape
    full = width * parts
    block = full // experts
    bits = bits_of(parts)[::-1]
    tap_count = taps_ref.shape[0]
    halo = extended.shape[0] - rows
    greet(
        [(lax.rem(me + k, experts), col) for k in range(1, experts)]
        + [(me, lax.rem(col + k, parts)) for k in range(1, parts)]
    )

    far_copy = remote(near_ref, far, far_sem.at[0], far_sem.at[1], (flipped(me, 1), col))
    far_copy.start()

    def part(column):
        return whole.at[pl.ds(pl.multiple_of(column * width, width), width), :]

    own = pltpu.make_async_copy(stream_ref, part(col), local_sem.at[0])
    own.start()
    index, held, copies = 0, [col], []
    for level, bit in enumerate(bits):
        for slot, column in enumerate(held):
            src = stream_ref if column is col else part(column)
            copy = remote(
                src, part(column), hop_send.at[index + slot], hop_recv.at[index + slot],
                (me, flipped(col, bit)),
            )
            copy.start()
            copies.append(copy)
        for slot in range(len(held)):
            column = flipped(held[slot], bit)
            remote(
                part(column), part(column), hop_send.at[index + slot], hop_recv.at[index + slot],
                (me, flipped(col, bit)),
            ).wait_recv()
        index += len(held)
        held = held + [flipped(column, bit) for column in held]
    own.wait()

    def piece(peer):
        return whole.at[pl.ds(pl.multiple_of(peer * block, block), block), :]

    def landing(receiver, source):
        slot = lax.rem(receiver + source, 2) * (experts // 2) + source // 2
        return arrived.at[:, pl.ds(pl.multiple_of(slot * rows, rows), rows)]

    def out_copy(peer):
        return remote(piece(peer), landing(peer, me), out_send.at[peer], out_recv.at[me], (peer, col))

    def start_out(k, carry):
        out_copy(lax.rem(me + k, experts)).start()
        return carry

    lax.fori_loop(1, experts, start_out, 0)
    mine = pltpu.make_async_copy(piece(me), landing(me, me), local_sem.at[1])
    mine.start()

    gain = gain_ref[...]
    rstd = column_of(rstd_ref[...], rows)
    swished_grad = lax.dot_general(
        whole[...], proj_ref[...], OUTER_DIMS, preferred_element_type=jnp.float32
    )
    normed = (conv_out_ref[...].astype(jnp.float32) - column_of(mean_ref[...], rows)) * rstd
    scaled = normed * gain
    sig = jax.nn.sigmoid(scaled)
    scaled_grad = swished_grad * sig * (1.0 + scaled * (1.0 - sig)) * gain
    grads[...] = scaled_grad
    norms[...] = normed
    first = jnp.sum(scaled_grad, axis=1, keepdims=True)
    second = jnp.sum(scaled_grad * normed, axis=1, keepdims=True)
    lane = lax.broadcasted_iota(jnp.int32, (rows, 128), 1)
    both = jnp.where(lane == 0, first, second)
    stats[parts] = both.T[:8]
    stat_copies = []
    for k in range(1, parts):
        copy = remote(
            stats.at[parts], stats.at[k], stat_send.at[k], stat_recv.at[k],
            (me, lax.rem(col + k, parts)),
        )
        copy.start()
        stat_copies.append(copy)
    for copy in stat_copies:
        copy.wait()
    total = stats[parts]
    for k in range(1, parts):
        total = total + stats[k]
    total = total / full
    spread = jnp.concatenate([total] * 16, axis=0).T
    first_mean = spread[:, 0:1]
    second_mean = spread[:, 1:2]
    extended[0:rows, :] = rstd * (grads[...] - first_mean - norms[...] * second_mean)

    def halo_copy(device):
        return remote(
            extended.at[pl.ds(0, halo), :], extended.at[pl.ds(rows, halo), :],
            halo_sem.at[0], halo_sem.at[1], (device, col),
        )

    @pl.when(me > 0)
    def _():
        halo_copy(lax.rem(me + experts - 1, experts)).start()

    @pl.when(me == experts - 1)
    def _():
        extended[rows:, :] = jnp.zeros((halo, width), jnp.float32)

    @pl.when(me < experts - 1)
    def _():
        halo_copy(lax.rem(me + experts - 1, experts)).wait_recv()

    for start in range(0, width, 128):
        cols = pl.ds(start, 128)
        total = jnp.zeros((rows, 128), jnp.float32)
        for offset in range(tap_count):
            total = total + taps_ref[offset : offset + 1, cols] * extended[pl.ds(offset, rows), cols]
        conv_ref[:, cols] = total.astype(jnp.bfloat16)

    def finish(k, carry):
        source = lax.rem(me - k + experts, experts)
        remote(
            piece(source), landing(me, source), out_send.at[source], out_recv.at[source], (source, col)
        ).wait_recv()
        out_copy(source).wait_send()
        return carry

    lax.fori_loop(1, experts, finish, 0)
    mine.wait()
    half = experts // 2 * rows
    proj_grad_ref[...] = jnp.dot(
        arrived[:, :half], near_ref[...].reshape(half, width), preferred_element_type=jnp.float32
    )
    far_copy.wait()
    proj_grad_ref[...] += jnp.dot(
        arrived[:, half:], far[...].reshape(half, width), preferred_element_type=jnp.float32
    )
    for copy in copies:
        copy.wait_send()

    @pl.when(me > 0)
    def _():
        halo_copy(lax.rem(me + experts - 1, experts)).wait_send()


def tail(stream_t, conv_out, mean, rstd, gain, taps, proj, near, experts, parts):
    width, rows = stream_t.shape
    full = width * parts
    block = full // experts
    halo = -(-(taps.shape[0] - 1) // 8) * 8
    return pl.pallas_call(
        functools.partial(tail_kernel, experts, parts),
        out_shape=(
            jax.ShapeDtypeStruct((rows, width), jnp.bfloat16),
            jax.ShapeDtypeStruct((block, width), jnp.float32),
        ),
        in_specs=[pl.BlockSpec(memory_space=VMEM)] * 8,
        out_specs=[pl.BlockSpec(memory_space=VMEM)] * 2,
        scratch_shapes=[
            VMEM((full, rows), jnp.bfloat16),
            VMEM((block, experts * rows), jnp.bfloat16),
            VMEM(near.shape, jnp.bfloat16),
            VMEM((rows + halo, width), jnp.float32),
            VMEM((parts + 1, 8, rows), jnp.float32),
            VMEM((rows, width), jnp.float32),
            VMEM((rows, width), jnp.float32),
            pltpu.SemaphoreType.DMA((parts - 1,)),
            pltpu.SemaphoreType.DMA((parts - 1,)),
            pltpu.SemaphoreType.DMA((experts,)),
            pltpu.SemaphoreType.DMA((experts,)),
            pltpu.SemaphoreType.DMA((parts,)),
            pltpu.SemaphoreType.DMA((parts,)),
            pltpu.SemaphoreType.DMA((2,)),
            pltpu.SemaphoreType.DMA((2,)),
            pltpu.SemaphoreType.DMA((2,)),
        ],
        compiler_params=pltpu.CompilerParams(collective_id=2, has_side_effects=True),
        name="tail",
    )(stream_t, conv_out, mean, rstd, gain, taps, proj, near)


def body(
    out_cotangent,
    expert_input,
    routes,
    route_weights,
    gate_proj,
    up_proj,
    down_proj,
    conv_out,
    conv_mean,
    conv_rstd,
    norm_gain,
    taps,
    out_proj,
):
    tok_rows = out_cotangent.shape[0]
    experts = lax.axis_size("sp")
    parts = lax.axis_size("tp")
    capacity = -(-3 * tok_rows // (experts * 16)) * 16
    slots = experts * capacity

    chosen = routes[:, :, None] == jnp.arange(experts, dtype=jnp.int32)[None, None, :]
    named = jnp.any(chosen, axis=1)
    weight = jnp.sum(jnp.where(chosen, route_weights[:, :, None], 0.0), axis=1)
    before = jnp.arange(tok_rows)[None, :] < jnp.arange(tok_rows)[:, None]
    rank = jnp.dot(
        before.astype(jnp.bfloat16), named.astype(jnp.bfloat16), preferred_element_type=jnp.float32
    ).astype(jnp.int32)
    rank = jnp.where(named, rank, -1)
    pick = rank.T[:, None, :] == jnp.arange(capacity, dtype=jnp.int32)[None, :, None]
    slot_weight = jnp.sum(jnp.where(pick, weight.T[:, None, :], 0.0), axis=2)
    pick = pick.astype(jnp.bfloat16).reshape(slots, tok_rows)
    send_rows = jnp.dot(pick, expert_input, preferred_element_type=jnp.float32).astype(jnp.bfloat16)
    send_cot = (
        jnp.dot(pick, out_cotangent, preferred_element_type=jnp.float32)
        * slot_weight.reshape(slots, 1)
    ).astype(jnp.bfloat16)
    mean, rstd, gain = conv_mean[None, :], conv_rstd[None, :], norm_gain[None, :]
    rows, cot, act, gate_back, up_back, stream, stream_t, near = front(
        send_rows, send_cot, pick.T, out_cotangent, conv_out, mean, rstd, gain,
        gate_proj, up_proj, down_proj, experts, parts,
    )
    conv_in_grad, proj_grad = tail(
        stream_t, conv_out, mean, rstd, gain, taps, out_proj, near, experts, parts
    )
    gate_grad, up_grad, down_grad = grads(rows, cot, act, gate_back, up_back)
    return (gate_grad, up_grad, down_grad, proj_grad, stream, conv_in_grad)


def solution(mesh):
    in_specs = (
        P("sp", "tp"),
        P("sp", "tp"),
        P("sp", None),
        P("sp", None),
        P("sp", None, "tp"),
        P("sp", None, "tp"),
        P("sp", "tp", None),
        P("sp", "tp"),
        P("sp"),
        P("sp"),
        P("tp"),
        P(None, "tp"),
        P(None, "tp"),
    )
    out_specs = (
        P("sp", None, "tp"),
        P("sp", None, "tp"),
        P("sp", "tp", None),
        P("sp", "tp"),
        P("sp", "tp"),
        P("sp", "tp"),
    )
    return jax.shard_map(body, mesh=mesh, in_specs=in_specs, out_specs=out_specs, check_vma=False)
```

```python
import functools

import jax
import jax.numpy as jnp
from jax import lax
from jax.experimental import pallas as pl
from jax.experimental.pallas import tpu as pltpu
from jax.sharding import PartitionSpec as P

OUTER_DIMS = (((0,), (0,)), ((), ()))
INNER_DIMS = (((1,), (1,)), ((), ()))
MESH = pl.DeviceIdType.MESH
VMEM = pltpu.VMEM


def flipped(index, bit):
    return index + bit - 2 * bit * ((index // bit) % 2)


def masked(index, mask):
    for bit in bits_of(mask + 1):
        if mask & bit:
            index = flipped(index, bit)
    return index


def bits_of(count):
    bits, bit = [], 1
    while bit < count:
        bits.append(bit)
        bit *= 2
    return bits


def greet(devices):
    barrier = pltpu.get_barrier_semaphore()
    for device in devices:
        pl.semaphore_signal(barrier, inc=1, device_id=device, device_id_type=MESH)
    pl.semaphore_wait(barrier, len(devices))


def remote(src, dst, send_sem, recv_sem, device):
    return pltpu.make_async_remote_copy(
        src_ref=src, dst_ref=dst, send_sem=send_sem, recv_sem=recv_sem,
        device_id=device, device_id_type=MESH,
    )


def column_of(row, rows):
    return jnp.broadcast_to(row, (128, rows)).T[:, 0:1]


def front_kernel(
    experts, parts, rows_send_ref, cot_send_ref, pick_ref, cotangent_ref, conv_out_ref, mean_ref,
    rstd_ref, gain_ref, gate_hbm, up_hbm, down_hbm,
    rows_out, cot_out, act_out, gate_out, up_out, stream_ref, stream_t_ref, near_ref,
    gate, up, down, full, gate_pre, up_pre, act_grad, backs, partial, first_recv, recv, work, final,
    routed, out_send, out_recv, hop_send, hop_recv, first_send, first_recv_sem, back_send, back_recv, home_send,
    home_recv, sw_send, sw_recv, weight_sem, save_sem, own_sem,
):
    me, col = lax.axis_index("sp"), lax.axis_index("tp")
    width = rows_send_ref.shape[1]
    capacity = rows_send_ref.shape[0] // experts
    hidden = gate.shape[1]
    tokens = conv_out_ref.shape[0]
    up_bits = bits_of(parts)
    bits = up_bits[::-1]
    levels = len(bits)
    loads = []
    for index, (src, dst) in enumerate(((gate_hbm, gate), (up_hbm, up), (down_hbm, down))):
        loads.append(pltpu.make_async_copy(src.at[0], dst, weight_sem.at[index]))
        loads[-1].start()
    greet(
        [(lax.rem(me + k, experts), col) for k in range(1, experts)]
        + [(me, flipped(col, bit)) for bit in bits]
    )
    sends = (rows_send_ref, cot_send_ref)

    def block_rows(source):
        return pl.ds(pl.multiple_of(source * capacity, capacity), capacity)

    def place(kind, source, column):
        return full.at[kind, column, block_rows(source), :]

    def out_copy(kind, peer, owner):
        return remote(
            sends[kind].at[block_rows(peer), :], place(kind, owner, col), out_send.at[kind, peer],
            out_recv.at[kind, owner], (peer, col),
        )

    held = [[col]]
    for bit in bits:
        held.append(held[-1] + [flipped(column, bit) for column in held[-1]])
    starts, total = [], 0
    for level in range(levels):
        starts.append(total)
        total += len(held[level])

    def hop(kind, level, slot, column, source, own=False):
        index = starts[level] + slot
        src = place(kind, source, column)
        if own:
            src = sends[kind].at[block_rows(me), :]
        return remote(
            src, place(kind, source, column),
            hop_send.at[kind, index, source], hop_recv.at[kind, index, source],
            (me, flipped(col, bits[level])),
        )

    def hop_arrival(kind, level, slot, source):
        return hop(kind, level, slot, flipped(held[level][slot], bits[level]), source)

    def first_hops(kind, source, own=False):
        for level in range(levels):
            hop(kind, level, 0, col, source, own).start()

    def arrive(kind, masks):
        for mask in masks:
            source = masked(me, mask)
            out_copy(kind, source, source).wait_recv()
            first_hops(kind, source)

    def pass_on(kind, masks):
        for level in range(1, levels):
            size = len(held[level - 1])
            for mask in masks:
                source = masked(me, mask)
                for slot in range(size):
                    hop_arrival(kind, level - 1, slot, source).wait_recv()
                for later in range(level, levels):
                    for slot in range(size, 2 * size):
                        hop(kind, later, slot, held[level][slot], source).start()

    def collect(kind, masks):
        for mask in masks:
            source = masked(me, mask)
            for slot in range(len(held[levels - 1])):
                hop_arrival(kind, levels - 1, slot, source).wait_recv()

    for kind in range(2):
        first_hops(kind, me, True)
    for kind in range(2):
        for mask in range(1, experts):
            peer = masked(me, mask)
            out_copy(kind, peer, me).start()
    own = []
    for kind in range(2):
        own.append(
            pltpu.make_async_copy(
                sends[kind].at[block_rows(me), :], place(kind, me, col), own_sem.at[kind]
            )
        )
        own[kind].start()
    for copy in own:
        copy.wait()

    scaled = (
        (conv_out_ref[...].astype(jnp.float32) - column_of(mean_ref[...], tokens))
        * column_of(rstd_ref[...], tokens)
        * gain_ref[...]
    )
    near_ref[me // 2] = (scaled * jax.nn.sigmoid(scaled)).astype(jnp.bfloat16)

    far_bits = bits_of(experts)[:0:-1]
    sources = [[me]]
    for bit in far_bits:
        sources.append(sources[-1] + [flipped(source, bit) for source in sources[-1]])

    def sw_copy(level, slot, source):
        index = (1 << level) - 1 + slot
        return remote(
            near_ref.at[source // 2], near_ref.at[source // 2], sw_send.at[index],
            sw_recv.at[index], (flipped(me, far_bits[level]), col),
        )

    def sw_start(level):
        for slot, source in enumerate(sources[level]):
            sw_copy(level, slot, source).start()

    def sw_arrive(level):
        for slot, source in enumerate(sources[level]):
            sw_copy(level, slot, flipped(source, far_bits[level])).wait_recv()

    def sw_pass():
        sw_arrive(0)
        if len(far_bits) > 1:
            sw_start(1)

    half = experts // 2
    near, far = list(range(half)), list(range(half, experts))
    own_half = me // half
    span = half * capacity

    def half_rows(side):
        index = own_half if side == 0 else 1 - own_half
        return pl.ds(pl.multiple_of(index * span, span), span)

    def joined(kind, rows):
        return jnp.concatenate([full[kind, part, rows, :] for part in range(parts)], axis=1)

    def pre(cols):
        rows = joined(0, slice(None))
        gate_pre[:, cols] = jnp.dot(rows, gate[:, cols], preferred_element_type=jnp.float32)
        up_pre[:, cols] = jnp.dot(rows, up[:, cols], preferred_element_type=jnp.float32)

    def back_tile(side, cols, size):
        act_grad[:, 0:size] = lax.dot_general(
            joined(1, half_rows(side)), down[cols, :], INNER_DIMS,
            preferred_element_type=jnp.float32,
        )
        base = (own_half if side == 0 else 1 - own_half) * half

        def chunk(k, carry):
            rows = block_rows(base + k)
            gates, ups, grad = gate_pre[rows, cols], up_pre[rows, cols], act_grad[block_rows(k), 0:size]
            sig = jax.nn.sigmoid(gates)
            silu = gates * sig
            backs[0, rows, cols] = (silu * ups).astype(jnp.bfloat16)
            backs[1, rows, cols] = (grad * ups * sig * (1.0 + gates * (1.0 - sig))).astype(
                jnp.bfloat16
            )
            backs[2, rows, cols] = (grad * silu).astype(jnp.bfloat16)
            return carry

        lax.fori_loop(0, half, chunk, 0)

    def back(side):
        def one(j, carry):
            back_tile(side, pl.ds(pl.multiple_of(j * 256, 256), 256), 256)
            return carry

        lax.fori_loop(0, hidden // 256, one, 0)
        if hidden % 256:
            back_tile(side, pl.ds(hidden - hidden % 256, hidden % 256), hidden % 256)

    arrive(0, range(1, experts))
    arrive(1, near[1:])
    pass_on(0, range(experts))
    collect(0, range(experts))
    loads[0].wait()
    loads[1].wait()
    tile_starts = list(range(0, hidden, 256))
    waiting = list(far)
    for index, start in enumerate(tile_starts):
        upto = len(far) * (index + 1) // len(tile_starts)
        arrive(1, far[len(far) - len(waiting) : upto])
        waiting = far[upto:]
        pre(pl.ds(start, min(256, hidden - start)))
    sw_start(0)
    pass_on(1, near)
    collect(1, near)
    loads[2].wait()
    back(0)

    kept = [[col]]
    for bit in bits:
        kept.insert(0, kept[0] + [flipped(column, bit) for column in kept[0]])
    order = near[1:] + far + [0]

    def first_copy(slot, side):
        rows = half_rows(side)
        return remote(
            partial.at[flipped(kept[1][slot], up_bits[0]), rows, :], first_recv.at[slot, rows, :],
            first_send.at[slot, side], first_recv_sem.at[slot, side],
            (me, flipped(col, up_bits[0])),
        )

    def fill(column, side):
        rows = pl.ds(pl.multiple_of(column * width, width), width)
        tokens_at = slice(None) if side is None else half_rows(side)
        value = lax.dot_general(
            backs[1, tokens_at, :], gate[rows, :], INNER_DIMS, preferred_element_type=jnp.float32
        ) + lax.dot_general(
            backs[2, tokens_at, :], up[rows, :], INNER_DIMS, preferred_element_type=jnp.float32
        )
        partial[column, tokens_at, :] = value.astype(jnp.bfloat16)

    back_starts, total = [0], 0
    for level in range(1, levels):
        back_starts.append(total)
        total += len(kept[level + 1])

    def back_copy(level, slot, block):
        index = back_starts[level] + slot
        return remote(
            work.at[index, block_rows(block), :], recv.at[index, block_rows(block), :],
            back_send.at[index, block], back_recv.at[index, block],
            (me, flipped(col, up_bits[level])),
        )

    def summed(level, slot, block):
        rows = block_rows(block)
        value = partial[kept[level][slot], rows, :].astype(jnp.float32)
        value = value + first_recv[slot, rows, :].astype(jnp.float32)
        for stage in range(1, level):
            value = value + recv[back_starts[stage] + slot, rows, :].astype(jnp.float32)
        return value.astype(jnp.bfloat16)

    size = len(kept[2]) if levels > 1 else 1
    late_slots = list(range(size, len(kept[1])))

    def fill_sent(side):
        for slot in late_slots:
            fill(flipped(kept[1][slot], up_bits[0]), side)
            first_copy(slot, side).start()
            fill(kept[1][slot], side)

    def send_sums(side):
        for slot in late_slots:
            first_copy(slot, side).wait_recv()
            for mask in (far if side else near):
                block = masked(me, mask)
                work[back_starts[1] + slot - size, block_rows(block), :] = summed(1, slot, block)
                back_copy(1, slot - size, block).start()

    fill_sent(0)
    pass_on(1, far)
    send_sums(0)
    collect(1, far)
    back(1)
    saves = [
        pltpu.make_async_copy(full.at[0], rows_out, save_sem.at[0]),
        pltpu.make_async_copy(full.at[1], cot_out, save_sem.at[1]),
        pltpu.make_async_copy(backs.at[0], act_out, save_sem.at[2]),
        pltpu.make_async_copy(backs.at[1], gate_out, save_sem.at[3]),
        pltpu.make_async_copy(backs.at[2], up_out, save_sem.at[4]),
    ]
    fill_sent(1)
    sw_pass()
    send_sums(1)
    for copy in saves:
        copy.start()
    for slot in reversed(range(size)):
        fill(flipped(kept[1][slot], up_bits[0]), None)
        for side in range(2):
            first_copy(slot, side).start()
        fill(kept[1][slot], None)
    for slot in range(size):
        for side in range(2):
            first_copy(slot, side).wait_recv()
    for level in range(2, levels):
        size = len(kept[level + 1])
        for mask in order:
            block = masked(me, mask)
            for slot in range(2 * size):
                back_copy(level - 1, slot, block).wait_recv()
            for slot in range(size):
                work[back_starts[level] + slot, block_rows(block), :] = summed(
                    level, size + slot, block
                )
                back_copy(level, slot, block).start()

    def home_copy(block, owner):
        return remote(
            final.at[block_rows(block), :], routed.at[block_rows(owner), :],
            home_send.at[block], home_recv.at[owner], (block, col),
        )

    for mask in order:
        block = masked(me, mask)
        if levels > 1:
            back_copy(levels - 1, 0, block).wait_recv()
        value = summed(levels, 0, block)
        if mask:
            final[block_rows(block), :] = value
            home_copy(block, me).start()
        else:
            routed[block_rows(block), :] = value
    for level in range(1, len(far_bits)):
        sw_arrive(level)
        if level + 1 < len(far_bits):
            sw_start(level + 1)
    for mask in order[:-1]:
        source = masked(me, mask)
        home_copy(source, source).wait_recv()
    stream = cotangent_ref[...].astype(jnp.float32) + jnp.dot(
        pick_ref[...], routed[...], preferred_element_type=jnp.float32
    )
    stream_ref[...] = stream.astype(jnp.bfloat16)
    stream_t_ref[...] = stream.T.astype(jnp.bfloat16)

    def finish(k, carry):
        source = lax.rem(me + k, experts)
        for kind in range(2):
            for level in range(levels):
                for slot in range(len(held[level])):
                    hop(kind, level, slot, held[level][slot], source).wait_send()
        for level in range(1, levels):
            for slot in range(len(kept[level + 1])):
                back_copy(level, slot, source).wait_send()

        @pl.when(k > 0)
        def _():
            for kind in range(2):
                out_copy(kind, source, me).wait_send()
            home_copy(source, me).wait_send()

        return carry

    lax.fori_loop(0, experts, finish, 0)
    for slot in range(len(kept[1])):
        for side in range(2):
            first_copy(slot, side).wait_send()
    for level in range(len(far_bits)):
        for slot, source in enumerate(sources[level]):
            sw_copy(level, slot, source).wait_send()
    for copy in saves:
        copy.wait()


def front(
    rows_send, cot_send, pick_t, cotangent, conv_out, mean, rstd, gain, gate, up, down, experts, parts
):
    slots, width = rows_send.shape
    full_width, hidden = gate.shape[1:]
    tokens = conv_out.shape[0]
    hops = parts - 1
    extra = max(parts // 2 - 1, 1)
    bf16, dma = jnp.bfloat16, pltpu.SemaphoreType.DMA
    rows_all = jax.ShapeDtypeStruct((parts, slots, width), bf16)
    acts = jax.ShapeDtypeStruct((slots, hidden), bf16)
    return pl.pallas_call(
        functools.partial(front_kernel, experts, parts),
        out_shape=(
            rows_all, rows_all, acts, acts, acts,
            jax.ShapeDtypeStruct((tokens, width), bf16),
            jax.ShapeDtypeStruct((width, tokens), bf16),
            jax.ShapeDtypeStruct((experts // 2, tokens, width), bf16),
        ),
        in_specs=[pl.BlockSpec(memory_space=VMEM)] * 8 + [pl.BlockSpec(memory_space=pl.ANY)] * 3,
        out_specs=[pl.BlockSpec(memory_space=pl.ANY)] * 5
        + [pl.BlockSpec(memory_space=VMEM)] * 3,
        scratch_shapes=[
            VMEM((full_width, hidden), bf16),
            VMEM((full_width, hidden), bf16),
            VMEM((hidden, full_width), bf16),
            VMEM((2, parts, slots, width), bf16),
            VMEM((slots, hidden), jnp.float32),
            VMEM((slots, hidden), jnp.float32),
            VMEM((slots // 2, 256), jnp.float32),
            VMEM((3, slots, hidden), bf16),
            VMEM((parts, slots, width), bf16),
            VMEM((max(parts // 2, 1), slots, width), bf16),
            VMEM((extra, slots, width), bf16),
            VMEM((extra, slots, width), bf16),
            VMEM((slots, width), bf16),
            VMEM((slots, width), bf16),
            dma((2, experts)),
            dma((2, experts)),
            dma((2, hops, experts)),
            dma((2, hops, experts)),
            dma((max(parts // 2, 1), 2)),
            dma((max(parts // 2, 1), 2)),
            dma((extra, experts)),
            dma((extra, experts)),
            dma((experts,)),
            dma((experts,)),
            dma((experts // 2,)),
            dma((experts // 2,)),
            dma((3,)),
            dma((5,)),
            dma((2,)),
        ],
        compiler_params=pltpu.CompilerParams(
            collective_id=0, has_side_effects=True, vmem_limit_bytes=67_000_000
        ),
        name="front",
    )(rows_send, cot_send, pick_t, cotangent, conv_out, mean, rstd, gain, gate, up, down)


def grads_kernel(rows_ref, cot_ref, act_ref, gate_ref, up_ref, gate_out, up_out, down_out):
    rows = rows_ref[...]
    gate_out[...] = lax.dot_general(
        rows, gate_ref[...], OUTER_DIMS, preferred_element_type=jnp.float32
    ).astype(jnp.bfloat16)
    up_out[...] = lax.dot_general(
        rows, up_ref[...], OUTER_DIMS, preferred_element_type=jnp.float32
    ).astype(jnp.bfloat16)
    down_out[...] = lax.dot_general(
        act_ref[...], cot_ref[...], OUTER_DIMS, preferred_element_type=jnp.float32
    ).astype(jnp.bfloat16)


def grads(rows, cot, act, gate_back, up_back):
    parts, slots, width = rows.shape
    hidden = act.shape[1]
    piece = pl.BlockSpec((None, slots, width), lambda i: (i, 0, 0))
    acts = pl.BlockSpec((slots, hidden), lambda i: (0, 0))
    across = pl.BlockSpec((None, width, hidden), lambda i: (0, i, 0))
    tall = jax.ShapeDtypeStruct((1, width * parts, hidden), jnp.bfloat16)
    return pl.pallas_call(
        grads_kernel,
        grid=(parts,),
        out_shape=(tall, tall, jax.ShapeDtypeStruct((1, hidden, width * parts), jnp.bfloat16)),
        in_specs=[piece, piece, acts, acts, acts],
        out_specs=[across, across, pl.BlockSpec((None, hidden, width), lambda i: (0, 0, i))],
        name="grads",
    )(rows, cot, act, gate_back, up_back)


def tail_kernel(
    experts, parts, stream_ref, conv_out_ref, mean_ref, rstd_ref, gain_ref, taps_ref, proj_ref,
    near_ref, conv_ref, proj_grad_ref,
    whole, arrived, far, extended, stats, grads, norms,
    hop_send, hop_recv, out_send, out_recv, stat_send, stat_recv, halo_sem, local_sem, far_sem,
):
    me, col = lax.axis_index("sp"), lax.axis_index("tp")
    width, rows = stream_ref.shape
    full = width * parts
    block = full // experts
    bits = bits_of(parts)[::-1]
    tap_count = taps_ref.shape[0]
    halo = extended.shape[0] - rows
    greet(
        [(lax.rem(me + k, experts), col) for k in range(1, experts)]
        + [(me, lax.rem(col + k, parts)) for k in range(1, parts)]
    )

    far_copy = remote(near_ref, far, far_sem.at[0], far_sem.at[1], (flipped(me, 1), col))
    far_copy.start()

    def part(column):
        return whole.at[pl.ds(pl.multiple_of(column * width, width), width), :]

    own = pltpu.make_async_copy(stream_ref, part(col), local_sem.at[0])
    own.start()
    index, held, copies = 0, [col], []
    for level, bit in enumerate(bits):
        for slot, column in enumerate(held):
            src = stream_ref if column is col else part(column)
            copy = remote(
                src, part(column), hop_send.at[index + slot], hop_recv.at[index + slot],
                (me, flipped(col, bit)),
            )
            copy.start()
            copies.append(copy)
        for slot in range(len(held)):
            column = flipped(held[slot], bit)
            remote(
                part(column), part(column), hop_send.at[index + slot], hop_recv.at[index + slot],
                (me, flipped(col, bit)),
            ).wait_recv()
        index += len(held)
        held = held + [flipped(column, bit) for column in held]
    own.wait()

    def piece(peer):
        return whole.at[pl.ds(pl.multiple_of(peer * block, block), block), :]

    def landing(receiver, source):
        slot = lax.rem(receiver + source, 2) * (experts // 2) + source // 2
        return arrived.at[:, pl.ds(pl.multiple_of(slot * rows, rows), rows)]

    def out_copy(peer):
        return remote(piece(peer), landing(peer, me), out_send.at[peer], out_recv.at[me], (peer, col))

    def start_out(k, carry):
        out_copy(lax.rem(me + k, experts)).start()
        return carry

    lax.fori_loop(1, experts, start_out, 0)
    mine = pltpu.make_async_copy(piece(me), landing(me, me), local_sem.at[1])
    mine.start()

    gain = gain_ref[...]
    rstd = column_of(rstd_ref[...], rows)
    swished_grad = lax.dot_general(
        whole[...], proj_ref[...], OUTER_DIMS, preferred_element_type=jnp.float32
    )
    normed = (conv_out_ref[...].astype(jnp.float32) - column_of(mean_ref[...], rows)) * rstd
    scaled = normed * gain
    sig = jax.nn.sigmoid(scaled)
    scaled_grad = swished_grad * sig * (1.0 + scaled * (1.0 - sig)) * gain
    grads[...] = scaled_grad
    norms[...] = normed
    first = jnp.sum(scaled_grad, axis=1, keepdims=True)
    second = jnp.sum(scaled_grad * normed, axis=1, keepdims=True)
    lane = lax.broadcasted_iota(jnp.int32, (rows, 128), 1)
    both = jnp.where(lane == 0, first, second)
    stats[parts] = both.T[:8]
    stat_copies = []
    for k in range(1, parts):
        copy = remote(
            stats.at[parts], stats.at[k], stat_send.at[k], stat_recv.at[k],
            (me, lax.rem(col + k, parts)),
        )
        copy.start()
        stat_copies.append(copy)
    for copy in stat_copies:
        copy.wait()
    total = stats[parts]
    for k in range(1, parts):
        total = total + stats[k]
    total = total / full
    spread = jnp.concatenate([total] * 16, axis=0).T
    first_mean = spread[:, 0:1]
    second_mean = spread[:, 1:2]
    extended[0:rows, :] = rstd * (grads[...] - first_mean - norms[...] * second_mean)

    def halo_copy(device):
        return remote(
            extended.at[pl.ds(0, halo), :], extended.at[pl.ds(rows, halo), :],
            halo_sem.at[0], halo_sem.at[1], (device, col),
        )

    @pl.when(me > 0)
    def _():
        halo_copy(lax.rem(me + experts - 1, experts)).start()

    @pl.when(me == experts - 1)
    def _():
        extended[rows:, :] = jnp.zeros((halo, width), jnp.float32)

    @pl.when(me < experts - 1)
    def _():
        halo_copy(lax.rem(me + experts - 1, experts)).wait_recv()

    for start in range(0, width, 128):
        cols = pl.ds(start, 128)
        total = jnp.zeros((rows, 128), jnp.float32)
        for offset in range(tap_count):
            total = total + taps_ref[offset : offset + 1, cols] * extended[pl.ds(offset, rows), cols]
        conv_ref[:, cols] = total.astype(jnp.bfloat16)

    def finish(k, carry):
        source = lax.rem(me - k + experts, experts)
        remote(
            piece(source), landing(me, source), out_send.at[source], out_recv.at[source], (source, col)
        ).wait_recv()
        out_copy(source).wait_send()
        return carry

    lax.fori_loop(1, experts, finish, 0)
    mine.wait()
    half = experts // 2 * rows
    proj_grad_ref[...] = jnp.dot(
        arrived[:, :half], near_ref[...].reshape(half, width), preferred_element_type=jnp.float32
    )
    far_copy.wait()
    proj_grad_ref[...] += jnp.dot(
        arrived[:, half:], far[...].reshape(half, width), preferred_element_type=jnp.float32
    )
    for copy in copies:
        copy.wait_send()

    @pl.when(me > 0)
    def _():
        halo_copy(lax.rem(me + experts - 1, experts)).wait_send()


def tail(stream_t, conv_out, mean, rstd, gain, taps, proj, near, experts, parts):
    width, rows = stream_t.shape
    full = width * parts
    block = full // experts
    halo = -(-(taps.shape[0] - 1) // 8) * 8
    return pl.pallas_call(
        functools.partial(tail_kernel, experts, parts),
        out_shape=(
            jax.ShapeDtypeStruct((rows, width), jnp.bfloat16),
            jax.ShapeDtypeStruct((block, width), jnp.float32),
        ),
        in_specs=[pl.BlockSpec(memory_space=VMEM)] * 8,
        out_specs=[pl.BlockSpec(memory_space=VMEM)] * 2,
        scratch_shapes=[
            VMEM((full, rows), jnp.bfloat16),
            VMEM((block, experts * rows), jnp.bfloat16),
            VMEM(near.shape, jnp.bfloat16),
            VMEM((rows + halo, width), jnp.float32),
            VMEM((parts + 1, 8, rows), jnp.float32),
            VMEM((rows, width), jnp.float32),
            VMEM((rows, width), jnp.float32),
            pltpu.SemaphoreType.DMA((parts - 1,)),
            pltpu.SemaphoreType.DMA((parts - 1,)),
            pltpu.SemaphoreType.DMA((experts,)),
            pltpu.SemaphoreType.DMA((experts,)),
            pltpu.SemaphoreType.DMA((parts,)),
            pltpu.SemaphoreType.DMA((parts,)),
            pltpu.SemaphoreType.DMA((2,)),
            pltpu.SemaphoreType.DMA((2,)),
            pltpu.SemaphoreType.DMA((2,)),
        ],
        compiler_params=pltpu.CompilerParams(
            collective_id=2, has_side_effects=True, vmem_limit_bytes=67_000_000
        ),
        name="tail",
    )(stream_t, conv_out, mean, rstd, gain, taps, proj, near)


def body(
    out_cotangent,
    expert_input,
    routes,
    route_weights,
    gate_proj,
    up_proj,
    down_proj,
    conv_out,
    conv_mean,
    conv_rstd,
    norm_gain,
    taps,
    out_proj,
):
    tok_rows = out_cotangent.shape[0]
    experts = lax.axis_size("sp")
    parts = lax.axis_size("tp")
    capacity = -(-3 * tok_rows // (experts * 16)) * 16
    slots = experts * capacity

    chosen = routes[:, :, None] == jnp.arange(experts, dtype=jnp.int32)[None, None, :]
    named = jnp.any(chosen, axis=1)
    weight = jnp.sum(jnp.where(chosen, route_weights[:, :, None], 0.0), axis=1)
    before = jnp.arange(tok_rows)[None, :] < jnp.arange(tok_rows)[:, None]
    rank = jnp.dot(
        before.astype(jnp.bfloat16), named.astype(jnp.bfloat16), preferred_element_type=jnp.float32
    ).astype(jnp.int32)
    rank = jnp.where(named, rank, -1)
    pick = rank.T[:, None, :] == jnp.arange(capacity, dtype=jnp.int32)[None, :, None]
    slot_weight = jnp.sum(jnp.where(pick, weight.T[:, None, :], 0.0), axis=2)
    pick = pick.astype(jnp.bfloat16).reshape(slots, tok_rows)
    send_rows = jnp.dot(pick, expert_input, preferred_element_type=jnp.float32).astype(jnp.bfloat16)
    send_cot = (
        jnp.dot(pick, out_cotangent, preferred_element_type=jnp.float32)
        * slot_weight.reshape(slots, 1)
    ).astype(jnp.bfloat16)
    mean, rstd, gain = conv_mean[None, :], conv_rstd[None, :], norm_gain[None, :]
    rows, cot, act, gate_back, up_back, stream, stream_t, near = front(
        send_rows, send_cot, pick.T, out_cotangent, conv_out, mean, rstd, gain,
        gate_proj, up_proj, down_proj, experts, parts,
    )
    conv_in_grad, proj_grad = tail(
        stream_t, conv_out, mean, rstd, gain, taps, out_proj, near, experts, parts
    )
    gate_grad, up_grad, down_grad = grads(rows, cot, act, gate_back, up_back)
    return (gate_grad, up_grad, down_grad, proj_grad, stream, conv_in_grad)


def solution(mesh):
    in_specs = (
        P("sp", "tp"),
        P("sp", "tp"),
        P("sp", None),
        P("sp", None),
        P("sp", None, "tp"),
        P("sp", None, "tp"),
        P("sp", "tp", None),
        P("sp", "tp"),
        P("sp"),
        P("sp"),
        P("tp"),
        P(None, "tp"),
        P(None, "tp"),
    )
    out_specs = (
        P("sp", None, "tp"),
        P("sp", None, "tp"),
        P("sp", "tp", None),
        P("sp", "tp"),
        P("sp", "tp"),
        P("sp", "tp"),
    )
    return jax.shard_map(body, mesh=mesh, in_specs=in_specs, out_specs=out_specs, check_vma=False)
```

```python
import functools

import jax
import jax.numpy as jnp
from jax import lax
from jax.experimental import pallas as pl
from jax.experimental.pallas import tpu as pltpu
from jax.sharding import PartitionSpec as P

OUTER_DIMS = (((0,), (0,)), ((), ()))
INNER_DIMS = (((1,), (1,)), ((), ()))
MESH = pl.DeviceIdType.MESH
VMEM = pltpu.VMEM


def flipped(index, bit):
    return index + bit - 2 * bit * ((index // bit) % 2)


def masked(index, mask):
    for bit in bits_of(mask + 1):
        if mask & bit:
            index = flipped(index, bit)
    return index


def bits_of(count):
    bits, bit = [], 1
    while bit < count:
        bits.append(bit)
        bit *= 2
    return bits


def hail(devices):
    barrier = pltpu.get_barrier_semaphore()
    for device in devices:
        pl.semaphore_signal(barrier, inc=1, device_id=device, device_id_type=MESH)


def gather_hails(count):
    pl.semaphore_wait(pltpu.get_barrier_semaphore(), count)


def remote(src, dst, send_sem, recv_sem, device):
    return pltpu.make_async_remote_copy(
        src_ref=src, dst_ref=dst, send_sem=send_sem, recv_sem=recv_sem,
        device_id=device, device_id_type=MESH,
    )


def column_of(row, rows):
    return jnp.broadcast_to(row, (128, rows)).T[:, 0:1]


def step_kernel(
    experts, parts, tokens_ref, cotangent_ref, routes_ref, weights_ref, conv_out_ref, mean_ref,
    rstd_ref, gain_ref, taps_ref, gate_hbm, up_hbm, down_hbm, proj_hbm,
    rows_out, cot_out, act_out, gate_out, up_out, stream_ref, conv_ref, proj_grad_ref,
    pick, rows_send_ref, cot_send_ref, gate, up, down, proj, full, gate_pre, up_pre, act_grad, backs,
    partial, first_recv, recv, work, final, routed, swish, stream_t, whole, arrived, grads, scaled_norm,
    extended, halo_grads, halo_norms, stats, next_stats,
    out_send, out_recv, hop_send, hop_recv, first_send, first_recv_sem, back_send,
    back_recv, home_send, home_recv, sw_send, sw_recv, side_send, side_recv, ring_send, ring_recv,
    piece_send, piece_recv, twin_send, twin_recv, stat_send, stat_recv, next_send, next_recv,
    halo_sem, weight_sem, save_sem, own_sem,
):
    me, col = lax.axis_index("sp"), lax.axis_index("tp")
    tokens, width = tokens_ref.shape
    capacity = pick.shape[0] // experts
    hidden = gate.shape[1]
    piece = width * parts // experts
    per_column = width // piece
    halo = halo_grads.shape[0]
    up_bits = bits_of(parts)
    bits = up_bits[::-1]
    levels = len(bits)
    loads = []
    for index, (src, dst) in enumerate(
        ((gate_hbm.at[0], gate), (up_hbm.at[0], up), (down_hbm.at[0], down), (proj_hbm, proj))
    ):
        loads.append(pltpu.make_async_copy(src, dst, weight_sem.at[index]))
        loads[-1].start()
    held = [[col]]
    for bit in bits:
        held.append(held[-1] + [flipped(column, bit) for column in held[-1]])
    twins = held[levels - 1]
    others = [flipped(column, bits[-1]) for column in twins]
    peers = [(lax.rem(me + k, experts), column) for k in range(1, experts) for column in twins]
    peers += [(me, column) for column in twins[1:] + others]
    peers += [(lax.rem(me + k, experts), column) for k in (1, experts - 1) for column in others]
    hail(peers)

    expert_at = lax.broadcasted_iota(jnp.int32, (experts, tokens), 0)
    first, second = routes_ref[0:1, :] == expert_at, routes_ref[1:2, :] == expert_at
    weight = jnp.where(first, weights_ref[0:1, :], 0.0) + jnp.where(second, weights_ref[1:2, :], 0.0)
    named = jnp.where(first | second, 1.0, 0.0)
    before = jnp.where(
        lax.broadcasted_iota(jnp.int32, (tokens, tokens), 0)
        < lax.broadcasted_iota(jnp.int32, (tokens, tokens), 1),
        1.0, 0.0,
    ).astype(jnp.bfloat16)
    rank = jnp.dot(named.astype(jnp.bfloat16), before, preferred_element_type=jnp.float32)
    rank = jnp.where(first | second, rank.astype(jnp.int32), -1)
    slot_at = lax.broadcasted_iota(jnp.int32, (capacity, tokens), 0)
    slot_weights = []
    for expert in range(experts):
        chosen = rank[expert : expert + 1, :] == slot_at
        pick[pl.ds(expert * capacity, capacity), :] = jnp.where(chosen, 1.0, 0.0).astype(jnp.bfloat16)
        slot_weights.append(
            jnp.sum(jnp.where(chosen, weight[expert : expert + 1, :], 0.0), axis=1, keepdims=True)
        )
    rows_send_ref[...] = jnp.dot(
        pick[...], tokens_ref[...], preferred_element_type=jnp.float32
    ).astype(jnp.bfloat16)
    for expert in range(experts):
        mine = pl.ds(expert * capacity, capacity)
        cot_send_ref[mine, :] = (
            jnp.dot(pick[mine, :], cotangent_ref[...], preferred_element_type=jnp.float32)
            * slot_weights[expert]
        ).astype(jnp.bfloat16)
    gather_hails(len(peers))
    sends = (rows_send_ref, cot_send_ref)

    def block_rows(source):
        return pl.ds(pl.multiple_of(source * capacity, capacity), capacity)

    def place(kind, source, column):
        return full.at[kind, column, block_rows(source), :]

    def out_copy(kind, peer, owner):
        return remote(
            sends[kind].at[block_rows(peer), :], place(kind, owner, col), out_send.at[kind, peer],
            out_recv.at[kind, owner], (peer, col),
        )

    starts, total = [], 0
    for level in range(levels):
        starts.append(total)
        total += len(held[level])

    def hop(kind, level, slot, column, source, own=False):
        index = starts[level] + slot
        src = place(kind, source, column)
        if own:
            src = sends[kind].at[block_rows(me), :]
        return remote(
            src, place(kind, source, column),
            hop_send.at[kind, index, source], hop_recv.at[kind, index, source],
            (me, flipped(col, bits[level])),
        )

    def hop_arrival(kind, level, slot, source):
        return hop(kind, level, slot, flipped(held[level][slot], bits[level]), source)

    def first_hops(kind, source, own=False):
        for level in range(levels):
            hop(kind, level, 0, col, source, own).start()

    def arrive(kind, masks):
        for mask in masks:
            source = masked(me, mask)
            out_copy(kind, source, source).wait_recv()
            first_hops(kind, source)

    def pass_on(kind, masks):
        for level in range(1, levels):
            size = len(held[level - 1])
            for mask in masks:
                source = masked(me, mask)
                for slot in range(size):
                    hop_arrival(kind, level - 1, slot, source).wait_recv()
                for later in range(level, levels):
                    for slot in range(size, 2 * size):
                        hop(kind, later, slot, held[level][slot], source).start()

    def collect(kind, masks):
        for mask in masks:
            source = masked(me, mask)
            for slot in range(len(held[levels - 1])):
                hop_arrival(kind, levels - 1, slot, source).wait_recv()

    for kind in range(2):
        first_hops(kind, me, True)
    for kind in range(2):
        for mask in range(1, experts):
            peer = masked(me, mask)
            out_copy(kind, peer, me).start()
    own = []
    for kind in range(2):
        own.append(
            pltpu.make_async_copy(
                sends[kind].at[block_rows(me), :], place(kind, me, col), own_sem.at[kind]
            )
        )
        own[kind].start()
    for copy in own:
        copy.wait()

    gain = gain_ref[...]
    rstd = column_of(rstd_ref[...], tokens)
    normed = (conv_out_ref[...].astype(jnp.float32) - column_of(mean_ref[...], tokens)) * rstd
    scaled = normed * gain
    swish[me] = (scaled * jax.nn.sigmoid(scaled)).astype(jnp.bfloat16)
    scaled_norm[...] = rstd * normed

    before_me = lax.rem(me + experts - 1, experts)

    def halo_copy(index, src, dst):
        return remote(
            src.at[pl.ds(0, halo), :], dst, halo_sem.at[index, 0], halo_sem.at[index, 1],
            (before_me, col),
        )

    @pl.when(me > 0)
    def _():
        halo_copy(0, scaled_norm, halo_norms).start()

    def side_copy(source):
        return remote(
            swish.at[source], swish.at[source], side_send.at[source], side_recv.at[source],
            (flipped(me, 1), col),
        )

    side_copy(me).start()

    far_bits = bits_of(experts)[:0:-1]
    sources = [[me]]
    for bit in far_bits:
        sources.append(sources[-1] + [flipped(source, bit) for source in sources[-1]])

    def sw_copy(level, slot, source):
        index = (1 << level) - 1 + slot
        return remote(
            swish.at[source], swish.at[source], sw_send.at[index],
            sw_recv.at[index], (flipped(me, far_bits[level]), col),
        )

    def sw_start(level):
        for slot, source in enumerate(sources[level]):
            sw_copy(level, slot, source).start()

    def sw_arrive(level):
        for slot, source in enumerate(sources[level]):
            sw_copy(level, slot, flipped(source, far_bits[level])).wait_recv()
            side_copy(flipped(source, far_bits[level])).start()

    def sw_pass():
        sw_arrive(0)
        if len(far_bits) > 1:
            sw_start(1)

    half = experts // 2
    near, far = list(range(half)), list(range(half, experts))
    own_half = me // half
    span = half * capacity

    def half_rows(side):
        index = own_half if side == 0 else 1 - own_half
        return pl.ds(pl.multiple_of(index * span, span), span)

    def joined(kind, rows):
        return jnp.concatenate([full[kind, part, rows, :] for part in range(parts)], axis=1)

    def pre(cols):
        rows = joined(0, slice(None))
        gate_pre[:, cols] = jnp.dot(rows, gate[:, cols], preferred_element_type=jnp.float32)
        up_pre[:, cols] = jnp.dot(rows, up[:, cols], preferred_element_type=jnp.float32)

    def back_tile(side, cols, size):
        act_grad[:, 0:size] = lax.dot_general(
            joined(1, half_rows(side)), down[cols, :], INNER_DIMS,
            preferred_element_type=jnp.float32,
        )
        base = (own_half if side == 0 else 1 - own_half) * half

        def chunk(k, carry):
            rows = block_rows(base + k)
            gates, ups, grad = gate_pre[rows, cols], up_pre[rows, cols], act_grad[block_rows(k), 0:size]
            sig = jax.nn.sigmoid(gates)
            silu = gates * sig
            backs[0, rows, cols] = (silu * ups).astype(jnp.bfloat16)
            backs[1, rows, cols] = (grad * ups * sig * (1.0 + gates * (1.0 - sig))).astype(
                jnp.bfloat16
            )
            backs[2, rows, cols] = (grad * silu).astype(jnp.bfloat16)
            return carry

        lax.fori_loop(0, half, chunk, 0)

    def back(side):
        def one(j, carry):
            back_tile(side, pl.ds(pl.multiple_of(j * 256, 256), 256), 256)
            return carry

        lax.fori_loop(0, hidden // 256, one, 0)
        if hidden % 256:
            back_tile(side, pl.ds(hidden - hidden % 256, hidden % 256), hidden % 256)

    arrive(0, range(1, experts))
    arrive(1, near[1:])
    pass_on(0, range(experts))
    collect(0, range(experts))
    loads[0].wait()
    loads[1].wait()
    tile_starts = list(range(0, hidden, 256))
    waiting = list(far)
    for index, start in enumerate(tile_starts):
        upto = len(far) * (index + 1) // len(tile_starts)
        arrive(1, far[len(far) - len(waiting) : upto])
        waiting = far[upto:]
        pre(pl.ds(start, min(256, hidden - start)))
    sw_start(0)
    pass_on(1, near)
    collect(1, near)
    loads[2].wait()
    back(0)

    kept = [[col]]
    for bit in bits:
        kept.insert(0, kept[0] + [flipped(column, bit) for column in kept[0]])
    order = near[1:] + far + [0]

    def first_copy(slot, side):
        rows = half_rows(side)
        return remote(
            partial.at[flipped(kept[1][slot], up_bits[0]), rows, :], first_recv.at[slot, rows, :],
            first_send.at[slot, side], first_recv_sem.at[slot, side],
            (me, flipped(col, up_bits[0])),
        )

    def fill(column, side):
        rows = pl.ds(pl.multiple_of(column * width, width), width)
        tokens_at = slice(None) if side is None else half_rows(side)
        value = lax.dot_general(
            backs[1, tokens_at, :], gate[rows, :], INNER_DIMS, preferred_element_type=jnp.float32
        ) + lax.dot_general(
            backs[2, tokens_at, :], up[rows, :], INNER_DIMS, preferred_element_type=jnp.float32
        )
        partial[column, tokens_at, :] = value.astype(jnp.bfloat16)

    back_starts, total = [0], 0
    for level in range(1, levels):
        back_starts.append(total)
        total += len(kept[level + 1])

    def back_copy(level, slot, block):
        index = back_starts[level] + slot
        return remote(
            work.at[index, block_rows(block), :], recv.at[index, block_rows(block), :],
            back_send.at[index, block], back_recv.at[index, block],
            (me, flipped(col, up_bits[level])),
        )

    def summed(level, slot, block):
        rows = block_rows(block)
        value = partial[kept[level][slot], rows, :].astype(jnp.float32)
        value = value + first_recv[slot, rows, :].astype(jnp.float32)
        for stage in range(1, level):
            value = value + recv[back_starts[stage] + slot, rows, :].astype(jnp.float32)
        return value.astype(jnp.bfloat16)

    size = len(kept[2]) if levels > 1 else 1
    late_slots = list(range(size, len(kept[1])))

    def fill_sent(side):
        for slot in late_slots:
            fill(flipped(kept[1][slot], up_bits[0]), side)
            first_copy(slot, side).start()
            fill(kept[1][slot], side)

    def send_sums(side):
        for slot in late_slots:
            first_copy(slot, side).wait_recv()
            for mask in (far if side else near):
                block = masked(me, mask)
                work[back_starts[1] + slot - size, block_rows(block), :] = summed(1, slot, block)
                back_copy(1, slot - size, block).start()

    fill_sent(0)
    pass_on(1, far)
    send_sums(0)
    collect(1, far)
    back(1)
    saves = [
        pltpu.make_async_copy(full.at[0], rows_out, save_sem.at[0]),
        pltpu.make_async_copy(full.at[1], cot_out, save_sem.at[1]),
        pltpu.make_async_copy(backs.at[0], act_out, save_sem.at[2]),
        pltpu.make_async_copy(backs.at[1], gate_out, save_sem.at[3]),
        pltpu.make_async_copy(backs.at[2], up_out, save_sem.at[4]),
    ]
    fill_sent(1)
    sw_pass()
    send_sums(1)
    for copy in saves:
        copy.start()
    for slot in reversed(range(size)):
        fill(flipped(kept[1][slot], up_bits[0]), None)
        for side in range(2):
            first_copy(slot, side).start()
        fill(kept[1][slot], None)
    for slot in range(size):
        for side in range(2):
            first_copy(slot, side).wait_recv()
    for level in range(2, levels):
        size = len(kept[level + 1])
        for mask in order:
            block = masked(me, mask)
            for slot in range(2 * size):
                back_copy(level - 1, slot, block).wait_recv()
            for slot in range(size):
                work[back_starts[level] + slot, block_rows(block), :] = summed(
                    level, size + slot, block
                )
                back_copy(level, slot, block).start()

    def home_copy(block, owner):
        return remote(
            final.at[block_rows(block), :], routed.at[block_rows(owner), :],
            home_send.at[block], home_recv.at[owner], (block, col),
        )

    for mask in order:
        block = masked(me, mask)
        if levels > 1:
            back_copy(levels - 1, 0, block).wait_recv()
        value = summed(levels, 0, block)
        if mask:
            final[block_rows(block), :] = value
            home_copy(block, me).start()
        else:
            routed[block_rows(block), :] = value
    for level in range(1, len(far_bits)):
        sw_arrive(level)
        if level + 1 < len(far_bits):
            sw_start(level + 1)
    for mask in order[:-1]:
        source = masked(me, mask)
        home_copy(source, source).wait_recv()
    stream = cotangent_ref[...].astype(jnp.float32) + lax.dot_general(
        pick[...], routed[...], OUTER_DIMS, preferred_element_type=jnp.float32
    )
    whole[col] = stream.astype(jnp.bfloat16)
    stream_t[...] = stream.T.astype(jnp.bfloat16)

    def ring(level, slot, column):
        index = starts[level] + slot
        return remote(
            whole.at[column], whole.at[column], ring_send.at[index], ring_recv.at[index],
            (me, flipped(col, bits[level])),
        )

    def ring_arrival(level, slot):
        return ring(level, slot, flipped(held[level][slot], bits[level]))

    for level in range(levels):
        ring(level, 0, col).start()

    def landing(source):
        return arrived.at[:, pl.ds(pl.multiple_of(source * tokens, tokens), tokens)]

    def piece_copy(j, slot, source, owner):
        index = j * len(twins) + slot
        return remote(
            stream_t.at[pl.ds(j * piece, piece), :], landing(owner), piece_send.at[index],
            piece_recv.at[source], (col * per_column + j, twins[slot]),
        )

    def own_piece(j):
        return pltpu.make_async_copy(
            stream_t.at[pl.ds(j * piece, piece), :], landing(me), own_sem.at[0]
        )

    for slot in reversed(range(len(twins))):
        for j in range(per_column):
            if slot:
                piece_copy(j, slot, me, me).start()
            else:

                @pl.when(col * per_column + j != me)
                def _(j=j):
                    piece_copy(j, 0, me, me).start()

                @pl.when(col * per_column + j == me)
                def _(j=j):
                    own_piece(j).start()
                    own_piece(j).wait()

    stream_ref[...] = stream.astype(jnp.bfloat16)
    loads[3].wait()

    def through(column):
        rows = pl.ds(pl.multiple_of(column * width, width), width)
        return jnp.dot(whole[column], proj[rows, :], preferred_element_type=jnp.float32)

    grads[...] = through(col)
    for level in range(1, levels):
        size = len(held[level - 1])
        for slot in range(size):
            ring_arrival(level - 1, slot).wait_recv()
        for later in range(level, levels):
            for slot in range(size, 2 * size):
                ring(later, slot, held[level][slot]).start()
        for slot in range(size):
            grads[...] += through(flipped(held[level - 1][slot], bits[level - 1]))
    for slot in range(len(held[levels - 1])):
        ring_arrival(levels - 1, slot).wait_recv()
        grads[...] += through(flipped(held[levels - 1][slot], bits[levels - 1]))
    gain = gain_ref[...]
    rstd = column_of(rstd_ref[...], tokens)
    normed = (conv_out_ref[...].astype(jnp.float32) - column_of(mean_ref[...], tokens)) * rstd
    scaled = normed * gain
    sig = jax.nn.sigmoid(scaled)
    scaled_grad = grads[...] * sig * (1.0 + scaled * (1.0 - sig)) * gain
    grads[...] = rstd * scaled_grad

    @pl.when(me > 0)
    def _():
        halo_copy(1, grads, halo_grads).start()

    first_sum = jnp.sum(scaled_grad, axis=1, keepdims=True)
    second_sum = jnp.sum(scaled_grad * normed, axis=1, keepdims=True)
    lane = lax.broadcasted_iota(jnp.int32, (tokens, 128), 1)
    table = jnp.where(lane == 0, first_sum, jnp.where(lane == 1, second_sum, rstd))
    stats[0] = table.T[:8]

    def stat_copy(k):
        return remote(
            stats.at[0], stats.at[k], stat_send.at[k], stat_recv.at[k],
            (me, lax.rem(col + k, parts)),
        )

    def next_copy(k):
        return remote(
            stats.at[0], next_stats.at[k], next_send.at[k], next_recv.at[k],
            (before_me, lax.rem(col + k, parts)),
        )

    for k in range(1, parts):
        stat_copy(k).start()

    @pl.when(me > 0)
    def _():
        for k in range(parts):
            next_copy(k).start()

    direct = lax.rem(me // per_column, 2) == lax.rem(col, 2)
    twin = flipped(col, 1)

    def twin_copy(source):
        return remote(
            landing(source), landing(source), twin_send.at[source], twin_recv.at[source], (me, twin)
        )

    @pl.when(direct)
    def _():
        for mask in range(experts):
            source = masked(me, mask)
            if mask:
                piece_copy(0, 0, source, source).wait_recv()
            else:

                @pl.when(me // per_column != col)
                def _():
                    piece_copy(0, 0, me, me).wait_recv()

            twin_copy(source).start()

    def means(refs):
        total = refs[0]
        for k in range(1, parts):
            total = total + refs[k]
        return jnp.concatenate([total / (width * parts)] * 16, axis=0).T

    for k in range(1, parts):
        stat_copy(k).wait_recv()
    spread = means(stats)
    extended[0:tokens, :] = (
        grads[...] - rstd * spread[:, 0:1] - scaled_norm[...] * spread[:, 1:2]
    )

    def conv(start, size):
        for lanes in range(0, width, 128):
            cols = pl.ds(lanes, 128)
            total = jnp.zeros((size, 128), jnp.float32)
            for offset in range(taps_ref.shape[0]):
                total = total + (
                    taps_ref[offset : offset + 1, cols] * extended[pl.ds(start + offset, size), cols]
                )
            conv_ref[pl.ds(start, size), cols] = total.astype(jnp.bfloat16)

    conv(0, tokens - halo)

    @pl.when(me == experts - 1)
    def _():
        extended[tokens:, :] = jnp.zeros((halo, width), jnp.float32)

    @pl.when(me < experts - 1)
    def _():
        halo_copy(0, scaled_norm, halo_norms).wait_recv()
        halo_copy(1, grads, halo_grads).wait_recv()
        for k in range(parts):
            next_copy(k).wait_recv()
        after = means(next_stats)[0:halo]
        extended[tokens:, :] = (
            halo_grads[...] - (after[:, 2:3] * width) * after[:, 0:1] - halo_norms[...] * after[:, 1:2]
        )

    conv(tokens - halo, halo)
    for source in sources[-1]:
        side_copy(flipped(source, 1)).wait_recv()

    @pl.when(jnp.logical_not(direct))
    def _():
        for mask in range(experts):
            twin_copy(masked(me, mask)).wait_recv()

    proj_grad_ref[...] = jnp.dot(
        arrived[...], swish[...].reshape(experts * tokens, width), preferred_element_type=jnp.float32
    )

    @pl.when(direct)
    def _():
        for mask in range(experts):
            twin_copy(masked(me, mask)).wait_send()

    for k in range(1, parts):
        stat_copy(k).wait_send()

    @pl.when(me > 0)
    def _():
        halo_copy(0, scaled_norm, halo_norms).wait_send()
        halo_copy(1, grads, halo_grads).wait_send()
        for k in range(parts):
            next_copy(k).wait_send()

    for level in range(levels):
        for slot in range(len(held[level])):
            ring(level, slot, held[level][slot]).wait_send()
    for slot in range(len(twins)):
        for j in range(per_column):
            if slot:
                piece_copy(j, slot, me, me).wait_send()
            else:

                @pl.when(col * per_column + j != me)
                def _(j=j):
                    piece_copy(j, 0, me, me).wait_send()

    for source in sources[-1]:
        side_copy(source).wait_send()

    def finish(k, carry):
        source = lax.rem(me + k, experts)
        for kind in range(2):
            for level in range(levels):
                for slot in range(len(held[level])):
                    hop(kind, level, slot, held[level][slot], source).wait_send()
        for level in range(1, levels):
            for slot in range(len(kept[level + 1])):
                back_copy(level, slot, source).wait_send()

        @pl.when(k > 0)
        def _():
            for kind in range(2):
                out_copy(kind, source, me).wait_send()
            home_copy(source, me).wait_send()

        return carry

    lax.fori_loop(0, experts, finish, 0)
    for slot in range(len(kept[1])):
        for side in range(2):
            first_copy(slot, side).wait_send()
    for level in range(len(far_bits)):
        for slot, source in enumerate(sources[level]):
            sw_copy(level, slot, source).wait_send()
    for copy in saves:
        copy.wait()


def step(
    tokens_in, cotangent, routes_t, weights_t, conv_out, mean, rstd, gain, taps, gate, up, down, proj,
    experts, parts,
):
    tokens, width = cotangent.shape
    slots = experts * (-(-3 * tokens // (experts * 16)) * 16)
    full_width, hidden = gate.shape[1:]
    block = full_width // experts
    halo = -(-(taps.shape[0] - 1) // 8) * 8
    hops = parts - 1
    half = max(parts // 2, 1)
    extra = max(half - 1, 1)
    bf16, f32, dma = jnp.bfloat16, jnp.float32, pltpu.SemaphoreType.DMA
    rows_all = jax.ShapeDtypeStruct((parts, slots, width), bf16)
    acts = jax.ShapeDtypeStruct((slots, hidden), bf16)
    in_vmem, anywhere = pl.BlockSpec(memory_space=VMEM), pl.BlockSpec(memory_space=pl.ANY)
    return pl.pallas_call(
        functools.partial(step_kernel, experts, parts),
        out_shape=(
            rows_all, rows_all, acts, acts, acts,
            jax.ShapeDtypeStruct((tokens, width), bf16),
            jax.ShapeDtypeStruct((tokens, width), bf16),
            jax.ShapeDtypeStruct((block, width), f32),
        ),
        in_specs=[in_vmem] * 9 + [anywhere] * 4,
        out_specs=[anywhere] * 5 + [in_vmem] * 3,
        scratch_shapes=[
            VMEM((slots, tokens), bf16),
            VMEM((slots, width), bf16),
            VMEM((slots, width), bf16),
            VMEM((full_width, hidden), bf16),
            VMEM((full_width, hidden), bf16),
            VMEM((hidden, full_width), bf16),
            VMEM((full_width, width), bf16),
            VMEM((2, parts, slots, width), bf16),
            VMEM((slots, hidden), f32),
            VMEM((slots, hidden), f32),
            VMEM((slots // 2, 256), f32),
            VMEM((3, slots, hidden), bf16),
            VMEM((parts, slots, width), bf16),
            VMEM((half, slots, width), bf16),
            VMEM((extra, slots, width), bf16),
            VMEM((extra, slots, width), bf16),
            VMEM((slots, width), bf16),
            VMEM((slots, width), bf16),
            VMEM((experts, tokens, width), bf16),
            VMEM((width, tokens), bf16),
            VMEM((parts, tokens, width), bf16),
            VMEM((block, experts * tokens), bf16),
            VMEM((tokens, width), f32),
            VMEM((tokens, width), f32),
            VMEM((tokens + halo, width), f32),
            VMEM((halo, width), f32),
            VMEM((halo, width), f32),
            VMEM((parts, 8, tokens), f32),
            VMEM((parts, 8, tokens), f32),
            dma((2, experts)),
            dma((2, experts)),
            dma((2, hops, experts)),
            dma((2, hops, experts)),
            dma((half, 2)),
            dma((half, 2)),
            dma((extra, experts)),
            dma((extra, experts)),
            dma((experts,)),
            dma((experts,)),
            dma((experts // 2,)),
            dma((experts // 2,)),
            dma((experts,)),
            dma((experts,)),
            dma((hops,)),
            dma((hops,)),
            dma((width // block * half,)),
            dma((experts,)),
            dma((experts,)),
            dma((experts,)),
            dma((parts,)),
            dma((parts,)),
            dma((parts,)),
            dma((parts,)),
            dma((2, 2)),
            dma((4,)),
            dma((5,)),
            dma((2,)),
        ],
        compiler_params=pltpu.CompilerParams(
            collective_id=0, has_side_effects=True, vmem_limit_bytes=67_000_000
        ),
        name="step",
    )(
        tokens_in, cotangent, routes_t, weights_t, conv_out, mean, rstd, gain, taps,
        gate, up, down, proj,
    )


def grads_kernel(rows_ref, cot_ref, act_ref, gate_ref, up_ref, gate_out, up_out, down_out):
    rows = rows_ref[...]
    gate_out[...] = lax.dot_general(
        rows, gate_ref[...], OUTER_DIMS, preferred_element_type=jnp.float32
    ).astype(jnp.bfloat16)
    up_out[...] = lax.dot_general(
        rows, up_ref[...], OUTER_DIMS, preferred_element_type=jnp.float32
    ).astype(jnp.bfloat16)
    down_out[...] = lax.dot_general(
        act_ref[...], cot_ref[...], OUTER_DIMS, preferred_element_type=jnp.float32
    ).astype(jnp.bfloat16)


def grads(rows, cot, act, gate_back, up_back):
    parts, slots, width = rows.shape
    hidden = act.shape[1]
    piece = pl.BlockSpec((None, slots, width), lambda i: (i, 0, 0))
    acts = pl.BlockSpec((slots, hidden), lambda i: (0, 0))
    across = pl.BlockSpec((None, width, hidden), lambda i: (0, i, 0))
    tall = jax.ShapeDtypeStruct((1, width * parts, hidden), jnp.bfloat16)
    return pl.pallas_call(
        grads_kernel,
        grid=(parts,),
        out_shape=(tall, tall, jax.ShapeDtypeStruct((1, hidden, width * parts), jnp.bfloat16)),
        in_specs=[piece, piece, acts, acts, acts],
        out_specs=[across, across, pl.BlockSpec((None, hidden, width), lambda i: (0, 0, i))],
        name="grads",
    )(rows, cot, act, gate_back, up_back)


def body(
    out_cotangent,
    expert_input,
    routes,
    route_weights,
    gate_proj,
    up_proj,
    down_proj,
    conv_out,
    conv_mean,
    conv_rstd,
    norm_gain,
    taps,
    out_proj,
):
    rows, cot, act, gate_back, up_back, stream, conv_in_grad, proj_grad = step(
        expert_input, out_cotangent, routes.T, route_weights.T, conv_out, conv_mean[None, :],
        conv_rstd[None, :], norm_gain[None, :], taps, gate_proj, up_proj, down_proj, out_proj,
        lax.axis_size("sp"), lax.axis_size("tp"),
    )
    gate_grad, up_grad, down_grad = grads(rows, cot, act, gate_back, up_back)
    return (gate_grad, up_grad, down_grad, proj_grad, stream, conv_in_grad)


def solution(mesh):
    in_specs = (
        P("sp", "tp"),
        P("sp", "tp"),
        P("sp", None),
        P("sp", None),
        P("sp", None, "tp"),
        P("sp", None, "tp"),
        P("sp", "tp", None),
        P("sp", "tp"),
        P("sp"),
        P("sp"),
        P("tp"),
        P(None, "tp"),
        P(None, "tp"),
    )
    out_specs = (
        P("sp", None, "tp"),
        P("sp", None, "tp"),
        P("sp", "tp", None),
        P("sp", "tp"),
        P("sp", "tp"),
        P("sp", "tp"),
    )
    return jax.shard_map(body, mesh=mesh, in_specs=in_specs, out_specs=out_specs, check_vma=False)
```

```python
import functools

import jax
import jax.numpy as jnp
from jax import lax
from jax.experimental import pallas as pl
from jax.experimental.pallas import tpu as pltpu
from jax.sharding import PartitionSpec as P

OUTER_DIMS = (((0,), (0,)), ((), ()))
INNER_DIMS = (((1,), (1,)), ((), ()))
MESH = pl.DeviceIdType.MESH
VMEM = pltpu.VMEM


def flipped(index, bit):
    return index + bit - 2 * bit * ((index // bit) % 2)


def masked(index, mask):
    for bit in bits_of(mask + 1):
        if mask & bit:
            index = flipped(index, bit)
    return index


def bits_of(count):
    bits, bit = [], 1
    while bit < count:
        bits.append(bit)
        bit *= 2
    return bits


def hail(devices):
    barrier = pltpu.get_barrier_semaphore()
    for device in devices:
        pl.semaphore_signal(barrier, inc=1, device_id=device, device_id_type=MESH)


def gather_hails(count):
    pl.semaphore_wait(pltpu.get_barrier_semaphore(), count)


def remote(src, dst, send_sem, recv_sem, device):
    return pltpu.make_async_remote_copy(
        src_ref=src, dst_ref=dst, send_sem=send_sem, recv_sem=recv_sem,
        device_id=device, device_id_type=MESH,
    )


def column_of(row, rows):
    return jnp.broadcast_to(row, (128, rows)).T[:, 0:1]


def step_kernel(
    experts, parts, tokens_ref, cotangent_ref, routes_ref, weights_ref, conv_out_ref, mean_ref,
    rstd_ref, gain_ref, taps_ref, gate_hbm, up_hbm, down_hbm, proj_hbm,
    rows_out, cot_out, act_out, gate_out, up_out, stream_ref, conv_ref, proj_grad_ref,
    pick, rows_send_ref, cot_send_ref, gate, up, down, proj, full, gate_pre, up_pre, act_grad, backs,
    partial, first_recv, recv, work, final, routed, swish, stream_t, whole, arrived, grads, scaled_norm,
    extended, halo_grads, halo_norms, stats, next_stats,
    out_send, out_recv, hop_send, hop_recv, first_send, first_recv_sem, back_send,
    back_recv, home_send, home_recv, sw_send, sw_recv, side_send, side_recv, ring_send, ring_recv,
    piece_send, piece_recv, twin_send, twin_recv, stat_send, stat_recv, next_send, next_recv,
    halo_sem, weight_sem, save_sem, own_sem,
):
    me, col = lax.axis_index("sp"), lax.axis_index("tp")
    tokens, width = tokens_ref.shape
    capacity = pick.shape[0] // experts
    hidden = gate.shape[1]
    piece = width * parts // experts
    per_column = width // piece
    halo = halo_grads.shape[0]
    up_bits = bits_of(parts)
    bits = up_bits[::-1]
    levels = len(bits)
    loads = []
    for index, (src, dst) in enumerate(
        ((gate_hbm.at[0], gate), (up_hbm.at[0], up), (down_hbm.at[0], down), (proj_hbm, proj))
    ):
        loads.append(pltpu.make_async_copy(src, dst, weight_sem.at[index]))
        loads[-1].start()
    held = [[col]]
    for bit in bits:
        held.append(held[-1] + [flipped(column, bit) for column in held[-1]])
    twins = held[levels - 1]
    others = [flipped(column, bits[-1]) for column in twins]
    peers = [(lax.rem(me + k, experts), column) for k in range(1, experts) for column in twins]
    peers += [(me, column) for column in twins[1:] + others]
    peers += [(lax.rem(me + k, experts), column) for k in (1, experts - 1) for column in others]
    hail(peers)

    expert_at = lax.broadcasted_iota(jnp.int32, (experts, tokens), 0)
    first, second = routes_ref[0:1, :] == expert_at, routes_ref[1:2, :] == expert_at
    weight = jnp.where(first, weights_ref[0:1, :], 0.0) + jnp.where(second, weights_ref[1:2, :], 0.0)
    named = jnp.where(first | second, 1.0, 0.0)
    before = jnp.where(
        lax.broadcasted_iota(jnp.int32, (tokens, tokens), 0)
        < lax.broadcasted_iota(jnp.int32, (tokens, tokens), 1),
        1.0, 0.0,
    ).astype(jnp.bfloat16)
    rank = jnp.dot(named.astype(jnp.bfloat16), before, preferred_element_type=jnp.float32)
    rank = jnp.where(first | second, rank.astype(jnp.int32), -1)
    slot_at = lax.broadcasted_iota(jnp.int32, (capacity, tokens), 0)
    slot_weights = []
    for expert in range(experts):
        chosen = rank[expert : expert + 1, :] == slot_at
        pick[pl.ds(expert * capacity, capacity), :] = jnp.where(chosen, 1.0, 0.0).astype(jnp.bfloat16)
        slot_weights.append(
            jnp.sum(jnp.where(chosen, weight[expert : expert + 1, :], 0.0), axis=1, keepdims=True)
        )
    rows_send_ref[...] = jnp.dot(
        pick[...], tokens_ref[...], preferred_element_type=jnp.float32
    ).astype(jnp.bfloat16)
    gather_hails(len(peers))
    sends = (rows_send_ref, cot_send_ref)

    def block_rows(source):
        return pl.ds(pl.multiple_of(source * capacity, capacity), capacity)

    def place(kind, source, column):
        return full.at[kind, column, block_rows(source), :]

    def out_copy(kind, peer, owner):
        return remote(
            sends[kind].at[block_rows(peer), :], place(kind, owner, col), out_send.at[kind, peer],
            out_recv.at[kind, owner], (peer, col),
        )

    starts, total = [], 0
    for level in range(levels):
        starts.append(total)
        total += len(held[level])

    def hop(kind, level, slot, column, source, own=False):
        index = starts[level] + slot
        src = place(kind, source, column)
        if own:
            src = sends[kind].at[block_rows(me), :]
        return remote(
            src, place(kind, source, column),
            hop_send.at[kind, index, source], hop_recv.at[kind, index, source],
            (me, flipped(col, bits[level])),
        )

    def hop_arrival(kind, level, slot, source):
        return hop(kind, level, slot, flipped(held[level][slot], bits[level]), source)

    def first_hops(kind, source, own=False):
        for level in range(levels):
            hop(kind, level, 0, col, source, own).start()

    def arrive(kind, masks):
        for mask in masks:
            source = masked(me, mask)
            out_copy(kind, source, source).wait_recv()
            first_hops(kind, source)

    def pass_on(kind, masks):
        for level in range(1, levels):
            size = len(held[level - 1])
            for mask in masks:
                source = masked(me, mask)
                for slot in range(size):
                    hop_arrival(kind, level - 1, slot, source).wait_recv()
                for later in range(level, levels):
                    for slot in range(size, 2 * size):
                        hop(kind, later, slot, held[level][slot], source).start()

    def collect(kind, masks):
        for mask in masks:
            source = masked(me, mask)
            for slot in range(len(held[levels - 1])):
                hop_arrival(kind, levels - 1, slot, source).wait_recv()

    half = experts // 2
    near, far = list(range(half)), list(range(half, experts))

    def leave(kind, masks):
        for mask in masks:
            out_copy(kind, masked(me, mask), me).start()

    first_hops(0, me, True)
    leave(0, near[1:])
    for expert in range(experts):
        mine = pl.ds(expert * capacity, capacity)
        cot_send_ref[mine, :] = (
            jnp.dot(pick[mine, :], cotangent_ref[...], preferred_element_type=jnp.float32)
            * slot_weights[expert]
        ).astype(jnp.bfloat16)
    first_hops(1, me, True)
    leave(1, near[1:])
    leave(0, far)
    leave(1, far)
    own = []
    for kind in range(2):
        own.append(
            pltpu.make_async_copy(
                sends[kind].at[block_rows(me), :], place(kind, me, col), own_sem.at[kind]
            )
        )
        own[kind].start()
    for copy in own:
        copy.wait()

    gain = gain_ref[...]
    rstd = column_of(rstd_ref[...], tokens)
    normed = (conv_out_ref[...].astype(jnp.float32) - column_of(mean_ref[...], tokens)) * rstd
    scaled = normed * gain
    swish[me] = (scaled * jax.nn.sigmoid(scaled)).astype(jnp.bfloat16)
    scaled_norm[...] = rstd * normed

    before_me = lax.rem(me + experts - 1, experts)

    def halo_copy(index, src, dst):
        return remote(
            src.at[pl.ds(0, halo), :], dst, halo_sem.at[index, 0], halo_sem.at[index, 1],
            (before_me, col),
        )

    @pl.when(me > 0)
    def _():
        halo_copy(0, scaled_norm, halo_norms).start()

    def side_copy(source):
        return remote(
            swish.at[source], swish.at[source], side_send.at[source], side_recv.at[source],
            (flipped(me, 1), col),
        )

    side_copy(me).start()

    far_bits = bits_of(experts)[:0:-1]
    sources = [[me]]
    for bit in far_bits:
        sources.append(sources[-1] + [flipped(source, bit) for source in sources[-1]])

    def sw_copy(level, slot, source):
        index = (1 << level) - 1 + slot
        return remote(
            swish.at[source], swish.at[source], sw_send.at[index],
            sw_recv.at[index], (flipped(me, far_bits[level]), col),
        )

    def sw_start(level):
        for slot, source in enumerate(sources[level]):
            sw_copy(level, slot, source).start()

    def sw_arrive(level):
        for slot, source in enumerate(sources[level]):
            sw_copy(level, slot, flipped(source, far_bits[level])).wait_recv()

    def sw_pass():
        sw_arrive(0)
        if len(far_bits) > 1:
            sw_start(1)

    own_half = me // half
    span = half * capacity

    def half_rows(side):
        index = own_half if side == 0 else 1 - own_half
        return pl.ds(pl.multiple_of(index * span, span), span)

    def joined(kind, rows):
        return jnp.concatenate([full[kind, part, rows, :] for part in range(parts)], axis=1)

    def pre(side, cols):
        at = half_rows(side)
        rows = joined(0, at)
        gate_pre[at, cols] = jnp.dot(rows, gate[:, cols], preferred_element_type=jnp.float32)
        up_pre[at, cols] = jnp.dot(rows, up[:, cols], preferred_element_type=jnp.float32)

    def back_tile(side, cols, size):
        act_grad[:, 0:size] = lax.dot_general(
            joined(1, half_rows(side)), down[cols, :], INNER_DIMS,
            preferred_element_type=jnp.float32,
        )
        base = (own_half if side == 0 else 1 - own_half) * half

        def chunk(k, carry):
            rows = block_rows(base + k)
            gates, ups, grad = gate_pre[rows, cols], up_pre[rows, cols], act_grad[block_rows(k), 0:size]
            sig = jax.nn.sigmoid(gates)
            silu = gates * sig
            backs[0, rows, cols] = (silu * ups).astype(jnp.bfloat16)
            backs[1, rows, cols] = (grad * ups * sig * (1.0 + gates * (1.0 - sig))).astype(
                jnp.bfloat16
            )
            backs[2, rows, cols] = (grad * silu).astype(jnp.bfloat16)
            return carry

        lax.fori_loop(0, half, chunk, 0)

    def back(side):
        def one(j, carry):
            back_tile(side, pl.ds(pl.multiple_of(j * 256, 256), 256), 256)
            return carry

        lax.fori_loop(0, hidden // 256, one, 0)
        if hidden % 256:
            back_tile(side, pl.ds(hidden - hidden % 256, hidden % 256), hidden % 256)

    kept = [[col]]
    for bit in bits:
        kept.insert(0, kept[0] + [flipped(column, bit) for column in kept[0]])
    order = far + near[1:] + [0]

    def first_copy(slot, side):
        rows = half_rows(side)
        return remote(
            partial.at[flipped(kept[1][slot], up_bits[0]), rows, :], first_recv.at[slot, rows, :],
            first_send.at[slot, side], first_recv_sem.at[slot, side],
            (me, flipped(col, up_bits[0])),
        )

    def fill(column, side):
        rows = pl.ds(pl.multiple_of(column * width, width), width)
        tokens_at = slice(None) if side is None else half_rows(side)
        value = lax.dot_general(
            backs[1, tokens_at, :], gate[rows, :], INNER_DIMS, preferred_element_type=jnp.float32
        ) + lax.dot_general(
            backs[2, tokens_at, :], up[rows, :], INNER_DIMS, preferred_element_type=jnp.float32
        )
        partial[column, tokens_at, :] = value.astype(jnp.bfloat16)

    back_starts, total = [0], 0
    for level in range(1, levels):
        back_starts.append(total)
        total += len(kept[level + 1])

    def back_copy(level, slot, block):
        index = back_starts[level] + slot
        return remote(
            work.at[index, block_rows(block), :], recv.at[index, block_rows(block), :],
            back_send.at[index, block], back_recv.at[index, block],
            (me, flipped(col, up_bits[level])),
        )

    def summed(level, slot, block):
        rows = block_rows(block)
        value = partial[kept[level][slot], rows, :].astype(jnp.float32)
        value = value + first_recv[slot, rows, :].astype(jnp.float32)
        for stage in range(1, level):
            value = value + recv[back_starts[stage] + slot, rows, :].astype(jnp.float32)
        return value.astype(jnp.bfloat16)

    size = len(kept[2]) if levels > 1 else 1
    late_slots = list(range(size, len(kept[1])))

    def fill_sent(side):
        for slot in late_slots:
            fill(flipped(kept[1][slot], up_bits[0]), side)
            first_copy(slot, side).start()
            fill(kept[1][slot], side)

    def send_sums(side):
        for slot in late_slots:
            first_copy(slot, side).wait_recv()
            for mask in (far if side else near):
                block = masked(me, mask)
                work[back_starts[1] + slot - size, block_rows(block), :] = summed(1, slot, block)
                back_copy(1, slot - size, block).start()

    def fill_kept(side):
        for slot in reversed(range(size)):
            fill(flipped(kept[1][slot], up_bits[0]), side)
            first_copy(slot, side).start()

    def fill_own(side):
        for slot in reversed(range(size)):
            fill(kept[1][slot], side)

    tile_starts = list(range(0, hidden, 256))

    def pre_near(start):
        pre(0, pl.ds(start, min(256, hidden - start)))

    def back_near(start):
        if start == 0:
            collect(1, near)
            loads[2].wait()
        size = min(256, hidden - start)
        back_tile(0, pl.ds(start, size), size)

    arrive(0, near[1:])
    arrive(1, near[1:])
    events = [(0, mask) for mask in far] + [(1, mask) for mask in far]
    ahead = len(far) // 2
    arrive(0, far[:ahead])
    pass_on(0, near)
    pass_on(1, near)
    collect(0, near)
    loads[0].wait()
    loads[1].wait()
    steps = [functools.partial(pre_near, start) for start in tile_starts]
    steps += [functools.partial(back_near, start) for start in tile_starts]
    steps += [functools.partial(fill_sent, 0), functools.partial(fill_kept, 0)]
    steps += [functools.partial(fill_own, 0)]
    done = 0
    events = events[ahead:]
    for index, (kind, mask) in enumerate(events):
        arrive(kind, [mask])
        upto = len(steps) * (index + 1) // len(events)
        for task in steps[done:upto]:
            task()
        done = upto
    sw_start(0)
    pass_on(0, far)
    send_sums(0)
    collect(0, far)
    for start in tile_starts:
        pre(1, pl.ds(start, min(256, hidden - start)))
    pass_on(1, far)
    collect(1, far)
    sw_pass()
    back(1)
    saves = [
        pltpu.make_async_copy(full.at[0], rows_out, save_sem.at[0]),
        pltpu.make_async_copy(full.at[1], cot_out, save_sem.at[1]),
        pltpu.make_async_copy(backs.at[0], act_out, save_sem.at[2]),
        pltpu.make_async_copy(backs.at[1], gate_out, save_sem.at[3]),
        pltpu.make_async_copy(backs.at[2], up_out, save_sem.at[4]),
    ]
    fill_sent(1)
    fill_kept(1)
    send_sums(1)
    fill_own(1)
    for copy in saves:
        copy.start()
    for slot in range(size):
        for side in range(2):
            first_copy(slot, side).wait_recv()
    for level in range(2, levels):
        size = len(kept[level + 1])
        for mask in order:
            block = masked(me, mask)
            for slot in range(2 * size):
                back_copy(level - 1, slot, block).wait_recv()
            for slot in range(size):
                work[back_starts[level] + slot, block_rows(block), :] = summed(
                    level, size + slot, block
                )
                back_copy(level, slot, block).start()

    def home_copy(block, owner):
        return remote(
            final.at[block_rows(block), :], routed.at[block_rows(owner), :],
            home_send.at[block], home_recv.at[owner], (block, col),
        )

    for mask in order:
        block = masked(me, mask)
        if levels > 1:
            back_copy(levels - 1, 0, block).wait_recv()
        value = summed(levels, 0, block)
        if mask:
            final[block_rows(block), :] = value
            home_copy(block, me).start()
        else:
            routed[block_rows(block), :] = value
    for level in range(1, len(far_bits)):
        sw_arrive(level)
        if level + 1 < len(far_bits):
            sw_start(level + 1)
    for source in sources[-1][1:]:
        side_copy(source).start()
    for mask in order[:-1]:
        source = masked(me, mask)
        home_copy(source, source).wait_recv()
    stream = cotangent_ref[...].astype(jnp.float32) + lax.dot_general(
        pick[...], routed[...], OUTER_DIMS, preferred_element_type=jnp.float32
    )
    whole[col] = stream.astype(jnp.bfloat16)
    stream_t[...] = stream.T.astype(jnp.bfloat16)

    def ring(level, slot, column):
        index = starts[level] + slot
        return remote(
            whole.at[column], whole.at[column], ring_send.at[index], ring_recv.at[index],
            (me, flipped(col, bits[level])),
        )

    def ring_arrival(level, slot):
        return ring(level, slot, flipped(held[level][slot], bits[level]))

    for level in range(levels):
        ring(level, 0, col).start()

    def landing(source):
        return arrived.at[:, pl.ds(pl.multiple_of(source * tokens, tokens), tokens)]

    def piece_copy(j, slot, source, owner):
        index = j * len(twins) + slot
        return remote(
            stream_t.at[pl.ds(j * piece, piece), :], landing(owner), piece_send.at[index],
            piece_recv.at[source], (col * per_column + j, twins[slot]),
        )

    def own_piece(j):
        return pltpu.make_async_copy(
            stream_t.at[pl.ds(j * piece, piece), :], landing(me), own_sem.at[0]
        )

    for slot in reversed(range(len(twins))):
        for j in range(per_column):
            if slot:
                piece_copy(j, slot, me, me).start()
            else:

                @pl.when(col * per_column + j != me)
                def _(j=j):
                    piece_copy(j, 0, me, me).start()

                @pl.when(col * per_column + j == me)
                def _(j=j):
                    own_piece(j).start()
                    own_piece(j).wait()

    stream_ref[...] = stream.astype(jnp.bfloat16)
    loads[3].wait()

    def through(column):
        rows = pl.ds(pl.multiple_of(column * width, width), width)
        return jnp.dot(whole[column], proj[rows, :], preferred_element_type=jnp.float32)

    grads[...] = through(col)
    for level in range(1, levels):
        size = len(held[level - 1])
        for slot in range(size):
            ring_arrival(level - 1, slot).wait_recv()
        for later in range(level, levels):
            for slot in range(size, 2 * size):
                ring(later, slot, held[level][slot]).start()
        for slot in range(size):
            grads[...] += through(flipped(held[level - 1][slot], bits[level - 1]))
    for slot in range(len(held[levels - 1])):
        ring_arrival(levels - 1, slot).wait_recv()
        grads[...] += through(flipped(held[levels - 1][slot], bits[levels - 1]))
    gain = gain_ref[...]
    rstd = column_of(rstd_ref[...], tokens)
    normed = (conv_out_ref[...].astype(jnp.float32) - column_of(mean_ref[...], tokens)) * rstd
    scaled = normed * gain
    sig = jax.nn.sigmoid(scaled)
    scaled_grad = grads[...] * sig * (1.0 + scaled * (1.0 - sig)) * gain
    grads[...] = rstd * scaled_grad

    @pl.when(me > 0)
    def _():
        halo_copy(1, grads, halo_grads).start()

    first_sum = jnp.sum(scaled_grad, axis=1, keepdims=True)
    second_sum = jnp.sum(scaled_grad * normed, axis=1, keepdims=True)
    lane = lax.broadcasted_iota(jnp.int32, (tokens, 128), 1)
    table = jnp.where(lane == 0, first_sum, jnp.where(lane == 1, second_sum, rstd))
    stats[0] = table.T[:8]

    def stat_copy(k):
        return remote(
            stats.at[0], stats.at[k], stat_send.at[k], stat_recv.at[k],
            (me, lax.rem(col + k, parts)),
        )

    def next_copy(k):
        return remote(
            stats.at[0], next_stats.at[k], next_send.at[k], next_recv.at[k],
            (before_me, lax.rem(col + k, parts)),
        )

    for k in range(1, parts):
        stat_copy(k).start()

    @pl.when(me > 0)
    def _():
        for k in range(parts):
            next_copy(k).start()

    direct = lax.rem(me // per_column, 2) == lax.rem(col, 2)
    twin = flipped(col, 1)

    def twin_copy(source):
        return remote(
            landing(source), landing(source), twin_send.at[source], twin_recv.at[source], (me, twin)
        )

    @pl.when(direct)
    def _():
        for mask in range(experts):
            source = masked(me, mask)
            if mask:
                piece_copy(0, 0, source, source).wait_recv()
            else:

                @pl.when(me // per_column != col)
                def _():
                    piece_copy(0, 0, me, me).wait_recv()

            twin_copy(source).start()

    def means(refs):
        total = refs[0]
        for k in range(1, parts):
            total = total + refs[k]
        return jnp.concatenate([total / (width * parts)] * 16, axis=0).T

    for k in range(1, parts):
        stat_copy(k).wait_recv()
    spread = means(stats)
    extended[0:tokens, :] = (
        grads[...] - rstd * spread[:, 0:1] - scaled_norm[...] * spread[:, 1:2]
    )

    def conv(start, size):
        for lanes in range(0, width, 128):
            cols = pl.ds(lanes, 128)
            total = jnp.zeros((size, 128), jnp.float32)
            for offset in range(taps_ref.shape[0]):
                total = total + (
                    taps_ref[offset : offset + 1, cols] * extended[pl.ds(start + offset, size), cols]
                )
            conv_ref[pl.ds(start, size), cols] = total.astype(jnp.bfloat16)

    conv(0, tokens - halo)

    @pl.when(me == experts - 1)
    def _():
        extended[tokens:, :] = jnp.zeros((halo, width), jnp.float32)

    @pl.when(me < experts - 1)
    def _():
        halo_copy(0, scaled_norm, halo_norms).wait_recv()
        halo_copy(1, grads, halo_grads).wait_recv()
        for k in range(parts):
            next_copy(k).wait_recv()
        after = means(next_stats)[0:halo]
        extended[tokens:, :] = (
            halo_grads[...] - (after[:, 2:3] * width) * after[:, 0:1] - halo_norms[...] * after[:, 1:2]
        )

    conv(tokens - halo, halo)
    for source in sources[-1]:
        side_copy(flipped(source, 1)).wait_recv()

    @pl.when(jnp.logical_not(direct))
    def _():
        for mask in range(experts):
            twin_copy(masked(me, mask)).wait_recv()

    proj_grad_ref[...] = jnp.dot(
        arrived[...], swish[...].reshape(experts * tokens, width), preferred_element_type=jnp.float32
    )

    @pl.when(direct)
    def _():
        for mask in range(experts):
            twin_copy(masked(me, mask)).wait_send()

    for k in range(1, parts):
        stat_copy(k).wait_send()

    @pl.when(me > 0)
    def _():
        halo_copy(0, scaled_norm, halo_norms).wait_send()
        halo_copy(1, grads, halo_grads).wait_send()
        for k in range(parts):
            next_copy(k).wait_send()

    for level in range(levels):
        for slot in range(len(held[level])):
            ring(level, slot, held[level][slot]).wait_send()
    for slot in range(len(twins)):
        for j in range(per_column):
            if slot:
                piece_copy(j, slot, me, me).wait_send()
            else:

                @pl.when(col * per_column + j != me)
                def _(j=j):
                    piece_copy(j, 0, me, me).wait_send()

    for source in sources[-1]:
        side_copy(source).wait_send()

    def finish(k, carry):
        source = lax.rem(me + k, experts)
        for kind in range(2):
            for level in range(levels):
                for slot in range(len(held[level])):
                    hop(kind, level, slot, held[level][slot], source).wait_send()
        for level in range(1, levels):
            for slot in range(len(kept[level + 1])):
                back_copy(level, slot, source).wait_send()

        @pl.when(k > 0)
        def _():
            for kind in range(2):
                out_copy(kind, source, me).wait_send()
            home_copy(source, me).wait_send()

        return carry

    lax.fori_loop(0, experts, finish, 0)
    for slot in range(len(kept[1])):
        for side in range(2):
            first_copy(slot, side).wait_send()
    for level in range(len(far_bits)):
        for slot, source in enumerate(sources[level]):
            sw_copy(level, slot, source).wait_send()
    for copy in saves:
        copy.wait()


def step(
    tokens_in, cotangent, routes_t, weights_t, conv_out, mean, rstd, gain, taps, gate, up, down, proj,
    experts, parts,
):
    tokens, width = cotangent.shape
    slots = experts * (-(-3 * tokens // (experts * 16)) * 16)
    full_width, hidden = gate.shape[1:]
    block = full_width // experts
    halo = -(-(taps.shape[0] - 1) // 8) * 8
    hops = parts - 1
    half = max(parts // 2, 1)
    extra = max(half - 1, 1)
    bf16, f32, dma = jnp.bfloat16, jnp.float32, pltpu.SemaphoreType.DMA
    rows_all = jax.ShapeDtypeStruct((parts, slots, width), bf16)
    acts = jax.ShapeDtypeStruct((slots, hidden), bf16)
    in_vmem, anywhere = pl.BlockSpec(memory_space=VMEM), pl.BlockSpec(memory_space=pl.ANY)
    return pl.pallas_call(
        functools.partial(step_kernel, experts, parts),
        out_shape=(
            rows_all, rows_all, acts, acts, acts,
            jax.ShapeDtypeStruct((tokens, width), bf16),
            jax.ShapeDtypeStruct((tokens, width), bf16),
            jax.ShapeDtypeStruct((block, width), f32),
        ),
        in_specs=[in_vmem] * 9 + [anywhere] * 4,
        out_specs=[anywhere] * 5 + [in_vmem] * 3,
        scratch_shapes=[
            VMEM((slots, tokens), bf16),
            VMEM((slots, width), bf16),
            VMEM((slots, width), bf16),
            VMEM((full_width, hidden), bf16),
            VMEM((full_width, hidden), bf16),
            VMEM((hidden, full_width), bf16),
            VMEM((full_width, width), bf16),
            VMEM((2, parts, slots, width), bf16),
            VMEM((slots, hidden), f32),
            VMEM((slots, hidden), f32),
            VMEM((slots // 2, 256), f32),
            VMEM((3, slots, hidden), bf16),
            VMEM((parts, slots, width), bf16),
            VMEM((half, slots, width), bf16),
            VMEM((extra, slots, width), bf16),
            VMEM((extra, slots, width), bf16),
            VMEM((slots, width), bf16),
            VMEM((slots, width), bf16),
            VMEM((experts, tokens, width), bf16),
            VMEM((width, tokens), bf16),
            VMEM((parts, tokens, width), bf16),
            VMEM((block, experts * tokens), bf16),
            VMEM((tokens, width), f32),
            VMEM((tokens, width), f32),
            VMEM((tokens + halo, width), f32),
            VMEM((halo, width), f32),
            VMEM((halo, width), f32),
            VMEM((parts, 8, tokens), f32),
            VMEM((parts, 8, tokens), f32),
            dma((2, experts)),
            dma((2, experts)),
            dma((2, hops, experts)),
            dma((2, hops, experts)),
            dma((half, 2)),
            dma((half, 2)),
            dma((extra, experts)),
            dma((extra, experts)),
            dma((experts,)),
            dma((experts,)),
            dma((experts // 2,)),
            dma((experts // 2,)),
            dma((experts,)),
            dma((experts,)),
            dma((hops,)),
            dma((hops,)),
            dma((width // block * half,)),
            dma((experts,)),
            dma((experts,)),
            dma((experts,)),
            dma((parts,)),
            dma((parts,)),
            dma((parts,)),
            dma((parts,)),
            dma((2, 2)),
            dma((4,)),
            dma((5,)),
            dma((2,)),
        ],
        compiler_params=pltpu.CompilerParams(
            collective_id=0, has_side_effects=True, vmem_limit_bytes=67_000_000
        ),
        name="step",
    )(
        tokens_in, cotangent, routes_t, weights_t, conv_out, mean, rstd, gain, taps,
        gate, up, down, proj,
    )


def grads_kernel(
    rows_ref, cot_ref, act_ref, gate_ref, up_ref, stream_ref, conv_ref, proj_ref,
    gate_out, up_out, down_out, stream_out, conv_out, proj_out, act_t,
):
    stream_out[...] = stream_ref[...]
    conv_out[...] = conv_ref[...]
    proj_out[...] = proj_ref[...]

    @pl.when(pl.program_id(0) == 0)
    def _():
        act_t[...] = act_ref[...].T

    rows_t = rows_ref[...].T
    gate_out[...] = jnp.dot(
        rows_t, gate_ref[...], preferred_element_type=jnp.float32
    ).astype(jnp.bfloat16)
    up_out[...] = jnp.dot(
        rows_t, up_ref[...], preferred_element_type=jnp.float32
    ).astype(jnp.bfloat16)
    down_out[...] = jnp.dot(
        act_t[...], cot_ref[...], preferred_element_type=jnp.float32
    ).astype(jnp.bfloat16)


def grads(rows, cot, act, gate_back, up_back, stream, conv, proj):
    parts, slots, width = rows.shape
    hidden = act.shape[1]
    piece = pl.BlockSpec((None, slots, width), lambda i: (i, 0, 0))
    acts = pl.BlockSpec((slots, hidden), lambda i: (0, 0))
    across = pl.BlockSpec((None, width, hidden), lambda i: (0, i, 0))
    tall = jax.ShapeDtypeStruct((1, width * parts, hidden), jnp.bfloat16)

    def strip(array):
        return pl.BlockSpec((array.shape[0] // parts, array.shape[1]), lambda i: (i, 0))

    passed = (stream, conv, proj)
    return pl.pallas_call(
        grads_kernel,
        grid=(parts,),
        out_shape=(tall, tall, jax.ShapeDtypeStruct((1, hidden, width * parts), jnp.bfloat16))
        + tuple(jax.ShapeDtypeStruct(array.shape, array.dtype) for array in passed),
        in_specs=[piece, piece, acts, acts, acts] + [strip(array) for array in passed],
        out_specs=[across, across, pl.BlockSpec((None, hidden, width), lambda i: (0, 0, i))]
        + [strip(array) for array in passed],
        scratch_shapes=[VMEM((hidden, slots), jnp.bfloat16)],
        name="grads",
    )(rows, cot, act, gate_back, up_back, *passed)


def body(
    out_cotangent,
    expert_input,
    routes,
    route_weights,
    gate_proj,
    up_proj,
    down_proj,
    conv_out,
    conv_mean,
    conv_rstd,
    norm_gain,
    taps,
    out_proj,
):
    rows, cot, act, gate_back, up_back, stream, conv_in_grad, proj_grad = step(
        expert_input, out_cotangent, routes.T, route_weights.T, conv_out, conv_mean[None, :],
        conv_rstd[None, :], norm_gain[None, :], taps, gate_proj, up_proj, down_proj, out_proj,
        lax.axis_size("sp"), lax.axis_size("tp"),
    )
    gate_grad, up_grad, down_grad, stream, conv_in_grad, proj_grad = grads(
        rows, cot, act, gate_back, up_back, stream, conv_in_grad, proj_grad
    )
    return (gate_grad, up_grad, down_grad, proj_grad, stream, conv_in_grad)


def solution(mesh):
    in_specs = (
        P("sp", "tp"),
        P("sp", "tp"),
        P("sp", None),
        P("sp", None),
        P("sp", None, "tp"),
        P("sp", None, "tp"),
        P("sp", "tp", None),
        P("sp", "tp"),
        P("sp"),
        P("sp"),
        P("tp"),
        P(None, "tp"),
        P(None, "tp"),
    )
    out_specs = (
        P("sp", None, "tp"),
        P("sp", None, "tp"),
        P("sp", "tp", None),
        P("sp", "tp"),
        P("sp", "tp"),
        P("sp", "tp"),
    )
    return jax.shard_map(body, mesh=mesh, in_specs=in_specs, out_specs=out_specs, check_vma=False)
```

```python
import functools

import jax
import jax.numpy as jnp
from jax import lax
from jax.experimental import pallas as pl
from jax.experimental.pallas import tpu as pltpu
from jax.sharding import PartitionSpec as P

OUTER_DIMS = (((0,), (0,)), ((), ()))
INNER_DIMS = (((1,), (1,)), ((), ()))
MESH = pl.DeviceIdType.MESH
VMEM = pltpu.VMEM


def flipped(index, bit):
    return index + bit - 2 * bit * ((index // bit) % 2)


def masked(index, mask):
    for bit in bits_of(mask + 1):
        if mask & bit:
            index = flipped(index, bit)
    return index


def bits_of(count):
    bits, bit = [], 1
    while bit < count:
        bits.append(bit)
        bit *= 2
    return bits


def hail(devices):
    barrier = pltpu.get_barrier_semaphore()
    for device in devices:
        pl.semaphore_signal(barrier, inc=1, device_id=device, device_id_type=MESH)


def gather_hails(count):
    pl.semaphore_wait(pltpu.get_barrier_semaphore(), count)


def remote(src, dst, send_sem, recv_sem, device):
    return pltpu.make_async_remote_copy(
        src_ref=src, dst_ref=dst, send_sem=send_sem, recv_sem=recv_sem,
        device_id=device, device_id_type=MESH,
    )


def column_of(row, rows):
    return jnp.broadcast_to(row, (128, rows)).T[:, 0:1]


def step_kernel(
    experts, parts, tokens_ref, cotangent_ref, routes_ref, weights_ref, conv_out_ref, mean_ref,
    rstd_ref, gain_ref, taps_ref, gate_hbm, up_hbm, down_hbm, proj_hbm,
    rows_out, cot_out, act_out, gate_out, up_out, stream_ref, conv_ref, proj_grad_ref,
    pick, rows_send_ref, cot_send_ref, gate, up, down, proj, full, gate_pre, up_pre, act_grad, backs,
    partial, first_recv, recv, work, final, routed, swish, stream_t, whole, arrived, grads, scaled_norm,
    extended, halo_grads, halo_norms, stats, next_stats,
    out_send, out_recv, hop_send, hop_recv, first_send, first_recv_sem, back_send,
    back_recv, home_send, home_recv, sw_send, sw_recv, side_send, side_recv, ring_send, ring_recv,
    piece_send, piece_recv, twin_send, twin_recv, stat_send, stat_recv, next_send, next_recv,
    halo_sem, weight_sem, save_sem, own_sem,
):
    me, col = lax.axis_index("sp"), lax.axis_index("tp")
    tokens, width = tokens_ref.shape
    capacity = pick.shape[0] // experts
    hidden = gate.shape[1]
    piece = width * parts // experts
    per_column = width // piece
    halo = halo_grads.shape[0]
    up_bits = bits_of(parts)
    bits = up_bits[::-1]
    levels = len(bits)
    loads = []
    for index, (src, dst) in enumerate(
        ((gate_hbm.at[0], gate), (up_hbm.at[0], up), (down_hbm.at[0], down), (proj_hbm, proj))
    ):
        loads.append(pltpu.make_async_copy(src, dst, weight_sem.at[index]))
        loads[-1].start()
    held = [[col]]
    for bit in bits:
        held.append(held[-1] + [flipped(column, bit) for column in held[-1]])
    twins = held[levels - 1]
    others = [flipped(column, bits[-1]) for column in twins]
    peers = [(lax.rem(me + k, experts), column) for k in range(1, experts) for column in twins]
    peers += [(me, column) for column in twins[1:] + others]
    peers += [(lax.rem(me + k, experts), column) for k in (1, experts - 1) for column in others]
    hail(peers)

    expert_at = lax.broadcasted_iota(jnp.int32, (experts, tokens), 0)
    first, second = routes_ref[0:1, :] == expert_at, routes_ref[1:2, :] == expert_at
    weight = jnp.where(first, weights_ref[0:1, :], 0.0) + jnp.where(second, weights_ref[1:2, :], 0.0)
    named = jnp.where(first | second, 1.0, 0.0)
    before = jnp.where(
        lax.broadcasted_iota(jnp.int32, (tokens, tokens), 0)
        < lax.broadcasted_iota(jnp.int32, (tokens, tokens), 1),
        1.0, 0.0,
    ).astype(jnp.bfloat16)
    rank = jnp.dot(named.astype(jnp.bfloat16), before, preferred_element_type=jnp.float32)
    rank = jnp.where(first | second, rank.astype(jnp.int32), -1)
    slot_at = lax.broadcasted_iota(jnp.int32, (capacity, tokens), 0)
    slot_weights = []
    for expert in range(experts):
        chosen = rank[expert : expert + 1, :] == slot_at
        pick[pl.ds(expert * capacity, capacity), :] = jnp.where(chosen, 1.0, 0.0).astype(jnp.bfloat16)
        slot_weights.append(
            jnp.sum(jnp.where(chosen, weight[expert : expert + 1, :], 0.0), axis=1, keepdims=True)
        )
    rows_send_ref[...] = jnp.dot(
        pick[...], tokens_ref[...], preferred_element_type=jnp.float32
    ).astype(jnp.bfloat16)
    gather_hails(len(peers))
    sends = (rows_send_ref, cot_send_ref)

    def block_rows(source):
        return pl.ds(pl.multiple_of(source * capacity, capacity), capacity)

    def place(kind, source, column):
        return full.at[kind, column, block_rows(source), :]

    def out_copy(kind, peer, owner):
        return remote(
            sends[kind].at[block_rows(peer), :], place(kind, owner, col), out_send.at[kind, peer],
            out_recv.at[kind, owner], (peer, col),
        )

    starts, total = [], 0
    for level in range(levels):
        starts.append(total)
        total += len(held[level])

    def hop(kind, level, slot, column, source, own=False):
        index = starts[level] + slot
        src = place(kind, source, column)
        if own:
            src = sends[kind].at[block_rows(me), :]
        return remote(
            src, place(kind, source, column),
            hop_send.at[kind, index, source], hop_recv.at[kind, index, source],
            (me, flipped(col, bits[level])),
        )

    def hop_arrival(kind, level, slot, source):
        return hop(kind, level, slot, flipped(held[level][slot], bits[level]), source)

    def first_hops(kind, source, own=False):
        for level in range(levels):
            hop(kind, level, 0, col, source, own).start()

    def arrive(kind, masks):
        for mask in masks:
            source = masked(me, mask)
            out_copy(kind, source, source).wait_recv()
            first_hops(kind, source)

    def pass_on(kind, masks):
        for level in range(1, levels):
            size = len(held[level - 1])
            for mask in masks:
                source = masked(me, mask)
                for slot in range(size):
                    hop_arrival(kind, level - 1, slot, source).wait_recv()
                for later in range(level, levels):
                    for slot in range(size, 2 * size):
                        hop(kind, later, slot, held[level][slot], source).start()

    def collect(kind, masks):
        for mask in masks:
            source = masked(me, mask)
            for slot in range(len(held[levels - 1])):
                hop_arrival(kind, levels - 1, slot, source).wait_recv()

    half = experts // 2
    near, far = list(range(half)), list(range(half, experts))

    def leave(kind, masks):
        for mask in masks:
            out_copy(kind, masked(me, mask), me).start()

    first_hops(0, me, True)
    leave(0, near[1:])
    for expert in range(experts):
        mine = pl.ds(expert * capacity, capacity)
        cot_send_ref[mine, :] = (
            jnp.dot(pick[mine, :], cotangent_ref[...], preferred_element_type=jnp.float32)
            * slot_weights[expert]
        ).astype(jnp.bfloat16)
    first_hops(1, me, True)
    leave(1, near[1:])
    leave(0, far)
    leave(1, far)
    own = []
    for kind in range(2):
        own.append(
            pltpu.make_async_copy(
                sends[kind].at[block_rows(me), :], place(kind, me, col), own_sem.at[kind]
            )
        )
        own[kind].start()
    for copy in own:
        copy.wait()

    gain = gain_ref[...]
    rstd = column_of(rstd_ref[...], tokens)
    normed = (conv_out_ref[...].astype(jnp.float32) - column_of(mean_ref[...], tokens)) * rstd
    scaled = normed * gain
    swish[me] = (scaled * jax.nn.sigmoid(scaled)).astype(jnp.bfloat16)
    scaled_norm[...] = rstd * normed

    before_me = lax.rem(me + experts - 1, experts)

    def halo_copy(index, src, dst):
        return remote(
            src.at[pl.ds(0, halo), :], dst, halo_sem.at[index, 0], halo_sem.at[index, 1],
            (before_me, col),
        )

    @pl.when(me > 0)
    def _():
        halo_copy(0, scaled_norm, halo_norms).start()

    def side_copy(source):
        return remote(
            swish.at[source], swish.at[source], side_send.at[source], side_recv.at[source],
            (flipped(me, 1), col),
        )

    side_copy(me).start()

    far_bits = bits_of(experts)[:0:-1]
    sources = [[me]]
    for bit in far_bits:
        sources.append(sources[-1] + [flipped(source, bit) for source in sources[-1]])

    def sw_copy(level, slot, source):
        index = (1 << level) - 1 + slot
        return remote(
            swish.at[source], swish.at[source], sw_send.at[index],
            sw_recv.at[index], (flipped(me, far_bits[level]), col),
        )

    def sw_start(level):
        for slot, source in enumerate(sources[level]):
            sw_copy(level, slot, source).start()

    def sw_arrive(level):
        for slot, source in enumerate(sources[level]):
            sw_copy(level, slot, flipped(source, far_bits[level])).wait_recv()

    def sw_pass():
        sw_arrive(0)
        if len(far_bits) > 1:
            sw_start(1)

    own_half = me // half
    span = half * capacity

    def half_rows(side):
        index = own_half if side == 0 else 1 - own_half
        return pl.ds(pl.multiple_of(index * span, span), span)

    def joined(kind, rows):
        return jnp.concatenate([full[kind, part, rows, :] for part in range(parts)], axis=1)

    def pre(side, cols):
        at = half_rows(side)
        rows = joined(0, at)
        gate_pre[at, cols] = jnp.dot(rows, gate[:, cols], preferred_element_type=jnp.float32)
        up_pre[at, cols] = jnp.dot(rows, up[:, cols], preferred_element_type=jnp.float32)

    def back_tile(side, cols, size):
        grad = lax.dot_general(
            joined(1, half_rows(side)), down[cols, :], INNER_DIMS,
            preferred_element_type=jnp.float32,
        )
        at = half_rows(side)
        gates, ups = gate_pre[at, cols], up_pre[at, cols]
        sig = jax.nn.sigmoid(gates)
        silu = gates * sig
        backs[0, at, cols] = (silu * ups).astype(jnp.bfloat16)
        backs[1, at, cols] = (grad * ups * sig * (1.0 + gates * (1.0 - sig))).astype(jnp.bfloat16)
        backs[2, at, cols] = (grad * silu).astype(jnp.bfloat16)

    def back(side):
        for start in range(0, hidden, 256):
            size = min(256, hidden - start)
            back_tile(side, pl.ds(start, size), size)

    kept = [[col]]
    for bit in bits:
        kept.insert(0, kept[0] + [flipped(column, bit) for column in kept[0]])
    order = far + near[1:] + [0]

    def first_copy(slot, side):
        rows = half_rows(side)
        return remote(
            partial.at[flipped(kept[1][slot], up_bits[0]), rows, :], first_recv.at[slot, rows, :],
            first_send.at[slot, side], first_recv_sem.at[slot, side],
            (me, flipped(col, up_bits[0])),
        )

    def fill(column, side):
        rows = pl.ds(pl.multiple_of(column * width, width), width)
        tokens_at = slice(None) if side is None else half_rows(side)
        value = lax.dot_general(
            backs[1, tokens_at, :], gate[rows, :], INNER_DIMS, preferred_element_type=jnp.float32
        ) + lax.dot_general(
            backs[2, tokens_at, :], up[rows, :], INNER_DIMS, preferred_element_type=jnp.float32
        )
        partial[column, tokens_at, :] = value.astype(jnp.bfloat16)

    back_starts, total = [0], 0
    for level in range(1, levels):
        back_starts.append(total)
        total += len(kept[level + 1])

    def back_copy(level, slot, block):
        index = back_starts[level] + slot
        return remote(
            work.at[index, block_rows(block), :], recv.at[index, block_rows(block), :],
            back_send.at[index, block], back_recv.at[index, block],
            (me, flipped(col, up_bits[level])),
        )

    def summed(level, slot, block):
        rows = block_rows(block)
        value = partial[kept[level][slot], rows, :].astype(jnp.float32)
        value = value + first_recv[slot, rows, :].astype(jnp.float32)
        for stage in range(1, level):
            value = value + recv[back_starts[stage] + slot, rows, :].astype(jnp.float32)
        return value.astype(jnp.bfloat16)

    size = len(kept[2]) if levels > 1 else 1
    late_slots = list(range(size, len(kept[1])))

    def fill_sent(side):
        for slot in late_slots:
            fill(flipped(kept[1][slot], up_bits[0]), side)
            first_copy(slot, side).start()
            fill(kept[1][slot], side)

    def send_sums(side):
        for slot in late_slots:
            first_copy(slot, side).wait_recv()
            for mask in (far if side else near):
                block = masked(me, mask)
                work[back_starts[1] + slot - size, block_rows(block), :] = summed(1, slot, block)
                back_copy(1, slot - size, block).start()

    def fill_kept(side):
        for slot in reversed(range(size)):
            fill(flipped(kept[1][slot], up_bits[0]), side)
            first_copy(slot, side).start()

    def fill_own(side):
        for slot in reversed(range(size)):
            fill(kept[1][slot], side)

    tile_starts = list(range(0, hidden, 256))

    def pre_near(start):
        pre(0, pl.ds(start, min(256, hidden - start)))

    def back_near(start):
        if start == 0:
            collect(1, near)
            loads[2].wait()
        size = min(256, hidden - start)
        back_tile(0, pl.ds(start, size), size)

    arrive(0, near[1:])
    arrive(1, near[1:])
    events = [(0, mask) for mask in far] + [(1, mask) for mask in far]
    ahead = 3 * len(far) // 4
    arrive(0, far[:ahead])
    pass_on(0, near)
    pass_on(1, near)
    collect(0, near)
    loads[0].wait()
    loads[1].wait()
    steps = [functools.partial(pre_near, start) for start in tile_starts]
    steps += [functools.partial(back_near, start) for start in tile_starts]
    steps += [functools.partial(fill_sent, 0), functools.partial(fill_kept, 0)]
    steps += [functools.partial(fill_own, 0)]
    done = 0
    events = events[ahead:]
    for index, (kind, mask) in enumerate(events):
        arrive(kind, [mask])
        upto = len(steps) * (index + 1) // len(events)
        for task in steps[done:upto]:
            task()
        done = upto
    sw_start(0)
    pass_on(0, far)
    send_sums(0)
    collect(0, far)
    for start in tile_starts:
        pre(1, pl.ds(start, min(256, hidden - start)))
    pass_on(1, far)
    collect(1, far)
    sw_pass()
    back(1)
    saves = [
        pltpu.make_async_copy(full.at[0], rows_out, save_sem.at[0]),
        pltpu.make_async_copy(full.at[1], cot_out, save_sem.at[1]),
        pltpu.make_async_copy(backs.at[0], act_out, save_sem.at[2]),
        pltpu.make_async_copy(backs.at[1], gate_out, save_sem.at[3]),
        pltpu.make_async_copy(backs.at[2], up_out, save_sem.at[4]),
    ]
    fill_sent(1)
    fill_kept(1)
    send_sums(1)
    fill_own(1)
    for copy in saves:
        copy.start()
    for slot in range(size):
        for side in range(2):
            first_copy(slot, side).wait_recv()
    for level in range(2, levels):
        size = len(kept[level + 1])
        for mask in order:
            block = masked(me, mask)
            for slot in range(2 * size):
                back_copy(level - 1, slot, block).wait_recv()
            for slot in range(size):
                work[back_starts[level] + slot, block_rows(block), :] = summed(
                    level, size + slot, block
                )
                back_copy(level, slot, block).start()

    def home_copy(block, owner):
        return remote(
            final.at[block_rows(block), :], routed.at[block_rows(owner), :],
            home_send.at[block], home_recv.at[owner], (block, col),
        )

    for mask in order:
        block = masked(me, mask)
        if levels > 1:
            back_copy(levels - 1, 0, block).wait_recv()
        value = summed(levels, 0, block)
        if mask:
            final[block_rows(block), :] = value
            home_copy(block, me).start()
        else:
            routed[block_rows(block), :] = value
    for level in range(1, len(far_bits)):
        sw_arrive(level)
        if level + 1 < len(far_bits):
            sw_start(level + 1)
    for source in sources[-1][1:]:
        side_copy(source).start()
    for mask in order[:-1]:
        source = masked(me, mask)
        home_copy(source, source).wait_recv()
    stream = cotangent_ref[...].astype(jnp.float32) + lax.dot_general(
        pick[...], routed[...], OUTER_DIMS, preferred_element_type=jnp.float32
    )
    whole[col] = stream.astype(jnp.bfloat16)
    stream_t[...] = stream.T.astype(jnp.bfloat16)

    def ring(level, slot, column):
        index = starts[level] + slot
        return remote(
            whole.at[column], whole.at[column], ring_send.at[index], ring_recv.at[index],
            (me, flipped(col, bits[level])),
        )

    def ring_arrival(level, slot):
        return ring(level, slot, flipped(held[level][slot], bits[level]))

    for level in range(levels):
        ring(level, 0, col).start()

    def landing(source):
        return arrived.at[:, pl.ds(pl.multiple_of(source * tokens, tokens), tokens)]

    def piece_copy(j, slot, source, owner):
        index = j * len(twins) + slot
        return remote(
            stream_t.at[pl.ds(j * piece, piece), :], landing(owner), piece_send.at[index],
            piece_recv.at[source], (col * per_column + j, twins[slot]),
        )

    def own_piece(j):
        return pltpu.make_async_copy(
            stream_t.at[pl.ds(j * piece, piece), :], landing(me), own_sem.at[0]
        )

    for slot in reversed(range(len(twins))):
        for j in range(per_column):
            if slot:
                piece_copy(j, slot, me, me).start()
            else:

                @pl.when(col * per_column + j != me)
                def _(j=j):
                    piece_copy(j, 0, me, me).start()

                @pl.when(col * per_column + j == me)
                def _(j=j):
                    own_piece(j).start()
                    own_piece(j).wait()

    stream_ref[...] = stream.astype(jnp.bfloat16)
    loads[3].wait()

    def through(column):
        rows = pl.ds(pl.multiple_of(column * width, width), width)
        return jnp.dot(whole[column], proj[rows, :], preferred_element_type=jnp.float32)

    grads[...] = through(col)
    for level in range(1, levels):
        size = len(held[level - 1])
        for slot in range(size):
            ring_arrival(level - 1, slot).wait_recv()
        for later in range(level, levels):
            for slot in range(size, 2 * size):
                ring(later, slot, held[level][slot]).start()
        for slot in range(size):
            grads[...] += through(flipped(held[level - 1][slot], bits[level - 1]))
    for slot in range(len(held[levels - 1])):
        ring_arrival(levels - 1, slot).wait_recv()
        grads[...] += through(flipped(held[levels - 1][slot], bits[levels - 1]))
    gain = gain_ref[...]
    rstd = column_of(rstd_ref[...], tokens)
    normed = (conv_out_ref[...].astype(jnp.float32) - column_of(mean_ref[...], tokens)) * rstd
    scaled = normed * gain
    sig = jax.nn.sigmoid(scaled)
    scaled_grad = grads[...] * sig * (1.0 + scaled * (1.0 - sig)) * gain
    grads[...] = rstd * scaled_grad

    @pl.when(me > 0)
    def _():
        halo_copy(1, grads, halo_grads).start()

    first_sum = jnp.sum(scaled_grad, axis=1, keepdims=True)
    second_sum = jnp.sum(scaled_grad * normed, axis=1, keepdims=True)
    lane = lax.broadcasted_iota(jnp.int32, (tokens, 128), 1)
    table = jnp.where(lane == 0, first_sum, jnp.where(lane == 1, second_sum, rstd))
    stats[0] = table.T[:8]

    def stat_copy(k):
        return remote(
            stats.at[0], stats.at[k], stat_send.at[k], stat_recv.at[k],
            (me, lax.rem(col + k, parts)),
        )

    def next_copy(k):
        return remote(
            stats.at[0], next_stats.at[k], next_send.at[k], next_recv.at[k],
            (before_me, lax.rem(col + k, parts)),
        )

    for k in range(1, parts):
        stat_copy(k).start()

    @pl.when(me > 0)
    def _():
        for k in range(parts):
            next_copy(k).start()

    direct = lax.rem(me // per_column, 2) == lax.rem(col, 2)
    twin = flipped(col, 1)

    def twin_copy(source):
        return remote(
            landing(source), landing(source), twin_send.at[source], twin_recv.at[source], (me, twin)
        )

    @pl.when(direct)
    def _():
        for mask in range(experts):
            source = masked(me, mask)
            if mask:
                piece_copy(0, 0, source, source).wait_recv()
            else:

                @pl.when(me // per_column != col)
                def _():
                    piece_copy(0, 0, me, me).wait_recv()

            twin_copy(source).start()

    def means(refs):
        total = refs[0]
        for k in range(1, parts):
            total = total + refs[k]
        return jnp.concatenate([total / (width * parts)] * 16, axis=0).T

    for k in range(1, parts):
        stat_copy(k).wait_recv()
    spread = means(stats)
    extended[0:tokens, :] = (
        grads[...] - rstd * spread[:, 0:1] - scaled_norm[...] * spread[:, 1:2]
    )

    def conv(start, size):
        for lanes in range(0, width, 128):
            cols = pl.ds(lanes, 128)
            total = jnp.zeros((size, 128), jnp.float32)
            for offset in range(taps_ref.shape[0]):
                total = total + (
                    taps_ref[offset : offset + 1, cols] * extended[pl.ds(start + offset, size), cols]
                )
            conv_ref[pl.ds(start, size), cols] = total.astype(jnp.bfloat16)

    conv(0, tokens - halo)

    @pl.when(me == experts - 1)
    def _():
        extended[tokens:, :] = jnp.zeros((halo, width), jnp.float32)

    @pl.when(me < experts - 1)
    def _():
        halo_copy(0, scaled_norm, halo_norms).wait_recv()
        halo_copy(1, grads, halo_grads).wait_recv()
        for k in range(parts):
            next_copy(k).wait_recv()
        after = means(next_stats)[0:halo]
        extended[tokens:, :] = (
            halo_grads[...] - (after[:, 2:3] * width) * after[:, 0:1] - halo_norms[...] * after[:, 1:2]
        )

    conv(tokens - halo, halo)
    for source in sources[-1]:
        side_copy(flipped(source, 1)).wait_recv()

    @pl.when(jnp.logical_not(direct))
    def _():
        for mask in range(experts):
            twin_copy(masked(me, mask)).wait_recv()

    proj_grad_ref[...] = jnp.dot(
        arrived[...], swish[...].reshape(experts * tokens, width), preferred_element_type=jnp.float32
    )

    @pl.when(direct)
    def _():
        for mask in range(experts):
            twin_copy(masked(me, mask)).wait_send()

    for k in range(1, parts):
        stat_copy(k).wait_send()

    @pl.when(me > 0)
    def _():
        halo_copy(0, scaled_norm, halo_norms).wait_send()
        halo_copy(1, grads, halo_grads).wait_send()
        for k in range(parts):
            next_copy(k).wait_send()

    for level in range(levels):
        for slot in range(len(held[level])):
            ring(level, slot, held[level][slot]).wait_send()
    for slot in range(len(twins)):
        for j in range(per_column):
            if slot:
                piece_copy(j, slot, me, me).wait_send()
            else:

                @pl.when(col * per_column + j != me)
                def _(j=j):
                    piece_copy(j, 0, me, me).wait_send()

    for source in sources[-1]:
        side_copy(source).wait_send()

    def finish(k, carry):
        source = lax.rem(me + k, experts)
        for kind in range(2):
            for level in range(levels):
                for slot in range(len(held[level])):
                    hop(kind, level, slot, held[level][slot], source).wait_send()
        for level in range(1, levels):
            for slot in range(len(kept[level + 1])):
                back_copy(level, slot, source).wait_send()

        @pl.when(k > 0)
        def _():
            for kind in range(2):
                out_copy(kind, source, me).wait_send()
            home_copy(source, me).wait_send()

        return carry

    lax.fori_loop(0, experts, finish, 0)
    for slot in range(len(kept[1])):
        for side in range(2):
            first_copy(slot, side).wait_send()
    for level in range(len(far_bits)):
        for slot, source in enumerate(sources[level]):
            sw_copy(level, slot, source).wait_send()
    for copy in saves:
        copy.wait()


def step(
    tokens_in, cotangent, routes_t, weights_t, conv_out, mean, rstd, gain, taps, gate, up, down, proj,
    experts, parts,
):
    tokens, width = cotangent.shape
    slots = experts * (-(-3 * tokens // (experts * 16)) * 16)
    full_width, hidden = gate.shape[1:]
    block = full_width // experts
    halo = -(-(taps.shape[0] - 1) // 8) * 8
    hops = parts - 1
    half = max(parts // 2, 1)
    extra = max(half - 1, 1)
    bf16, f32, dma = jnp.bfloat16, jnp.float32, pltpu.SemaphoreType.DMA
    rows_all = jax.ShapeDtypeStruct((parts, slots, width), bf16)
    acts = jax.ShapeDtypeStruct((slots, hidden), bf16)
    in_vmem, anywhere = pl.BlockSpec(memory_space=VMEM), pl.BlockSpec(memory_space=pl.ANY)
    return pl.pallas_call(
        functools.partial(step_kernel, experts, parts),
        out_shape=(
            rows_all, rows_all, acts, acts, acts,
            jax.ShapeDtypeStruct((tokens, width), bf16),
            jax.ShapeDtypeStruct((tokens, width), bf16),
            jax.ShapeDtypeStruct((block, width), f32),
        ),
        in_specs=[in_vmem] * 9 + [anywhere] * 4,
        out_specs=[anywhere] * 5 + [in_vmem] * 3,
        scratch_shapes=[
            VMEM((slots, tokens), bf16),
            VMEM((slots, width), bf16),
            VMEM((slots, width), bf16),
            VMEM((full_width, hidden), bf16),
            VMEM((full_width, hidden), bf16),
            VMEM((hidden, full_width), bf16),
            VMEM((full_width, width), bf16),
            VMEM((2, parts, slots, width), bf16),
            VMEM((slots, hidden), f32),
            VMEM((slots, hidden), f32),
            VMEM((slots // 2, 256), f32),
            VMEM((3, slots, hidden), bf16),
            VMEM((parts, slots, width), bf16),
            VMEM((half, slots, width), bf16),
            VMEM((extra, slots, width), bf16),
            VMEM((extra, slots, width), bf16),
            VMEM((slots, width), bf16),
            VMEM((slots, width), bf16),
            VMEM((experts, tokens, width), bf16),
            VMEM((width, tokens), bf16),
            VMEM((parts, tokens, width), bf16),
            VMEM((block, experts * tokens), bf16),
            VMEM((tokens, width), f32),
            VMEM((tokens, width), f32),
            VMEM((tokens + halo, width), f32),
            VMEM((halo, width), f32),
            VMEM((halo, width), f32),
            VMEM((parts, 8, tokens), f32),
            VMEM((parts, 8, tokens), f32),
            dma((2, experts)),
            dma((2, experts)),
            dma((2, hops, experts)),
            dma((2, hops, experts)),
            dma((half, 2)),
            dma((half, 2)),
            dma((extra, experts)),
            dma((extra, experts)),
            dma((experts,)),
            dma((experts,)),
            dma((experts // 2,)),
            dma((experts // 2,)),
            dma((experts,)),
            dma((experts,)),
            dma((hops,)),
            dma((hops,)),
            dma((width // block * half,)),
            dma((experts,)),
            dma((experts,)),
            dma((experts,)),
            dma((parts,)),
            dma((parts,)),
            dma((parts,)),
            dma((parts,)),
            dma((2, 2)),
            dma((4,)),
            dma((5,)),
            dma((2,)),
        ],
        compiler_params=pltpu.CompilerParams(
            collective_id=0, has_side_effects=True, vmem_limit_bytes=67_000_000
        ),
        name="step",
    )(
        tokens_in, cotangent, routes_t, weights_t, conv_out, mean, rstd, gain, taps,
        gate, up, down, proj,
    )


def grads_kernel(
    rows_ref, cot_ref, act_ref, gate_ref, up_ref, stream_ref, conv_ref, proj_ref,
    gate_out, up_out, down_out, stream_out, conv_out, proj_out, act_t,
):
    stream_out[...] = stream_ref[...]
    conv_out[...] = conv_ref[...]
    proj_out[...] = proj_ref[...]

    @pl.when(pl.program_id(0) == 0)
    def _():
        act_t[...] = act_ref[...].T

    rows_t = rows_ref[...].T
    gate_out[...] = jnp.dot(
        rows_t, gate_ref[...], preferred_element_type=jnp.float32
    ).astype(jnp.bfloat16)
    up_out[...] = jnp.dot(
        rows_t, up_ref[...], preferred_element_type=jnp.float32
    ).astype(jnp.bfloat16)
    down_out[...] = jnp.dot(
        act_t[...], cot_ref[...], preferred_element_type=jnp.float32
    ).astype(jnp.bfloat16)


def grads(rows, cot, act, gate_back, up_back, stream, conv, proj):
    parts, slots, width = rows.shape
    hidden = act.shape[1]
    piece = pl.BlockSpec((None, slots, width), lambda i: (i, 0, 0))
    acts = pl.BlockSpec((slots, hidden), lambda i: (0, 0))
    across = pl.BlockSpec((None, width, hidden), lambda i: (0, i, 0))
    tall = jax.ShapeDtypeStruct((1, width * parts, hidden), jnp.bfloat16)

    def strip(array):
        return pl.BlockSpec((array.shape[0] // parts, array.shape[1]), lambda i: (i, 0))

    passed = (stream, conv, proj)
    return pl.pallas_call(
        grads_kernel,
        grid=(parts,),
        out_shape=(tall, tall, jax.ShapeDtypeStruct((1, hidden, width * parts), jnp.bfloat16))
        + tuple(jax.ShapeDtypeStruct(array.shape, array.dtype) for array in passed),
        in_specs=[piece, piece, acts, acts, acts] + [strip(array) for array in passed],
        out_specs=[across, across, pl.BlockSpec((None, hidden, width), lambda i: (0, 0, i))]
        + [strip(array) for array in passed],
        scratch_shapes=[VMEM((hidden, slots), jnp.bfloat16)],
        name="grads",
    )(rows, cot, act, gate_back, up_back, *passed)


def body(
    out_cotangent,
    expert_input,
    routes,
    route_weights,
    gate_proj,
    up_proj,
    down_proj,
    conv_out,
    conv_mean,
    conv_rstd,
    norm_gain,
    taps,
    out_proj,
):
    rows, cot, act, gate_back, up_back, stream, conv_in_grad, proj_grad = step(
        expert_input, out_cotangent, routes.T, route_weights.T, conv_out, conv_mean[None, :],
        conv_rstd[None, :], norm_gain[None, :], taps, gate_proj, up_proj, down_proj, out_proj,
        lax.axis_size("sp"), lax.axis_size("tp"),
    )
    gate_grad, up_grad, down_grad, stream, conv_in_grad, proj_grad = grads(
        rows, cot, act, gate_back, up_back, stream, conv_in_grad, proj_grad
    )
    return (gate_grad, up_grad, down_grad, proj_grad, stream, conv_in_grad)


def solution(mesh):
    in_specs = (
        P("sp", "tp"),
        P("sp", "tp"),
        P("sp", None),
        P("sp", None),
        P("sp", None, "tp"),
        P("sp", None, "tp"),
        P("sp", "tp", None),
        P("sp", "tp"),
        P("sp"),
        P("sp"),
        P("tp"),
        P(None, "tp"),
        P(None, "tp"),
    )
    out_specs = (
        P("sp", None, "tp"),
        P("sp", None, "tp"),
        P("sp", "tp", None),
        P("sp", "tp"),
        P("sp", "tp"),
        P("sp", "tp"),
    )
    return jax.shard_map(body, mesh=mesh, in_specs=in_specs, out_specs=out_specs, check_vma=False)
```
